512 devices in a mesh: sp: 64 (over z, y), tp: 8 (over x, core).
Axes of the slice: x: 4, y: 4, z: 16, core: 2. Of those that a mesh axis runs over, the one named last changes fastest.
Arguments:
- tokens: bfloat16 [4096, 4, 2048], P(('sp', 'tp')), may hold values from -16 to 16
- norm_gain: float32 [2048], replicated, may hold values from 0.1 to 1.9
- w_query: bfloat16 [2048, 2048], P('sp', 'tp'), may hold values from -0.125 to 0.125
- w_forget: bfloat16 [2048, 2048], P('sp', 'tp'), may hold values from -0.125 to 0.125
- w_value: bfloat16 [2048, 2048], P('sp', 'tp'), may hold values from -0.125 to 0.125
- floor_gap: float32 [2048], P('tp'), may hold values from 0 to 0.15, as said below
- head_gain: float32 [2048], P('tp'), may hold values from 0.1 to 1.9
- w_out: bfloat16 [2048, 2048], P('tp', 'sp'), may hold values from -0.125 to 0.125
Outputs:
- mixed: bfloat16 [4096, 4, 2048], P(('sp', 'tp'))
The draws below stay inside these ranges and needn't reach their ends.
Inputs may be any that keep to these rules, and one draw needn't show every extreme that they name: `floor_gap`: positive, at least 0.5 / 4096 and at most 0.15.
All inputs are finite; a program needn't handle non-finite values.
Results may differ from the reference program's by a relative error of at most 0.014.
Values may be sent and summed in bfloat16 or wider, within the bound.
No kernel may reach another device: no remote copies, remote signals or barrier semaphores. Data moves between devices by JAX's collectives and lax.ppermute only.
A program may use at most 128 MiB of HBM per device.

```python
import math
import jax
import jax.numpy as jnp
from jax import lax

D = 2048
HEADS = 16
KEY_DIM = 128
VAL_DIM = 128
SEQS = 4
HK = 2048
HV = 2048
LENGTH = 4096
N_TP = 8


def draw_tokens(key, part):
    noise_key, scale_key, aim_key, level_key = jax.random.split(key, 4)
    direction = jnp.clip(jax.random.normal(aim_key, (D,), jnp.float32), -4.0, 4.0)
    levels = jax.random.uniform(level_key, (LENGTH // 128 + 1, SEQS), jnp.float32, -2.5, 2.5)
    block_index = jnp.arange(LENGTH) // 128
    shift = levels[block_index][:, :, None] * direction
    base = jnp.clip(jax.random.normal(noise_key, (LENGTH, SEQS, D), jnp.float32), -6.0, 6.0)
    return (base + shift).astype(jnp.bfloat16)


def draw_floor_gap(key, part):
    kind_key, fast_key, slow_key = jax.random.split(jax.random.fold_in(key, 7), 3)
    slow_head = jax.random.randint(kind_key, (HEADS, 1), 0, 2) > 0
    fast_gap = jnp.exp(jax.random.uniform(fast_key, (HEADS, KEY_DIM), jnp.float32, math.log(0.04), math.log(0.145)))
    slow_gap = jnp.exp(jax.random.uniform(slow_key, (HEADS, KEY_DIM), jnp.float32, math.log(0.5), math.log(3.0))) / LENGTH
    return jnp.where(slow_head, slow_gap, fast_gap).reshape(HEADS * KEY_DIM).astype(jnp.float32)


def block_scale(own_key, extent, shards, low, largest):
    def one(position, blocks):
        draws = jax.random.uniform(jax.random.fold_in(jax.random.fold_in(own_key, 6), position), (blocks,), jnp.float32, low / len(shards), largest / len(shards))
        return jnp.repeat(jnp.exp(draws), extent[position] // blocks).reshape((-1,) + (1,) * (len(extent) - position - 1))

    level = one(*shards[0])
    for cut in shards[1:]:
        level = level * one(*cut)
    return level


def gaussian(key, shape, scale, reach, pieces=(), kind=jnp.bfloat16):
    result = jax.random.normal(key, shape, jnp.float32) * scale
    if len(pieces) > 0:
        result = block_scale(key, shape, pieces, -0.22, 0.18) * result
    return jnp.clip(result, min=-reach, max=reach).astype(kind)


def setup_inputs(seed: int = 0) -> dict:
    keys = jax.random.split(jax.random.key(seed), 9)
    tokens = draw_tokens(jax.random.fold_in(keys[8], 71), 0)
    norm_gain = jnp.clip(1.0 + 0.18 * jax.random.normal(keys[1], (D,), jnp.float32), 0.1, 1.9)
    w_query = gaussian(keys[2], (D, HK), D ** -0.5, 0.125, ((0, 64), (1, 8)))
    w_forget = gaussian(keys[3], (D, HK), D ** -0.5, 0.125, ((0, 64), (1, 8)))
    w_value = gaussian(keys[4], (D, HV), D ** -0.5, 0.125, ((0, 64), (1, 8)))
    floor_gap = draw_floor_gap(jax.random.fold_in(keys[8], 71), 0)
    head_gain = jnp.clip(1.0 + 0.18 * jax.random.normal(keys[6], (HV,), jnp.float32), 0.1, 1.9)
    w_out = gaussian(keys[7], (HV, D), HV ** -0.5, 0.125, ((0, 8), (1, 64)))
    return dict(tokens=tokens, norm_gain=norm_gain, w_query=w_query, w_forget=w_forget, w_value=w_value, floor_gap=floor_gap, head_gain=head_gain, w_out=w_out)


eps_norm = 1e-06
highest = lax.Precision.HIGHEST

def stored(value):
    return lax.optimization_barrier(value.astype(jnp.bfloat16)).astype(jnp.float32)

def reference(tokens, norm_gain, w_query, w_forget, w_value, floor_gap, head_gain, w_out):
    length, sequences = (tokens.shape[0], tokens.shape[1])
    flat = tokens.astype(jnp.float32)
    scale = lax.rsqrt(lax.optimization_barrier(jnp.mean(flat * flat, axis=-1, keepdims=True)) + eps_norm)
    normed = (flat * scale * norm_gain).astype(jnp.bfloat16).reshape(length * sequences, D)
    query_pre = stored(jnp.dot(normed, w_query, preferred_element_type=jnp.float32))
    forget_pre = stored(jnp.dot(normed, w_forget, preferred_element_type=jnp.float32))
    value_pre = stored(jnp.dot(normed, w_value, preferred_element_type=jnp.float32))
    block_len = math.gcd(length, 64)
    block_count = length // block_len

    def blocks(value, channels):
        return value.reshape(block_count, block_len, sequences, HEADS, channels)
    query = jax.nn.silu(blocks(query_pre, KEY_DIM))
    inkey = floor_gap.reshape(HEADS, KEY_DIM) * jax.nn.sigmoid(-blocks(forget_pre, KEY_DIM))
    log_forget = jnp.log1p(-inkey)
    values = blocks(value_pre, VAL_DIM)
    causal = jnp.tril(jnp.ones((block_len, block_len), dtype=bool))

    def advance(state, inputs):
        query_block, key_block, value_block, forget_block = inputs
        cumulative = jnp.cumsum(forget_block, axis=0)
        spread = cumulative[:, None] - cumulative[None, :]
        decay = jnp.exp(jnp.where(causal[:, :, None, None, None], spread, -jnp.inf))
        scores = jnp.einsum('tshk,ushk,tushk->shtu', query_block, key_block, decay, precision=highest)
        inside = jnp.einsum('shtu,ushv->tshv', scores, value_block, precision=highest)
        carried = jnp.einsum('tshk,shkv->tshv', query_block * jnp.exp(cumulative), state, precision=highest)
        final = cumulative[-1]
        weighted = key_block * jnp.exp(final[None] - cumulative)
        new_state = jnp.exp(final)[..., None] * state + jnp.einsum('ushk,ushv->shkv', weighted, value_block, precision=highest)
        return (new_state, inside + carried)
    start_state = jnp.zeros((sequences, HEADS, KEY_DIM, VAL_DIM), jnp.float32)
    _, recurrent = lax.scan(advance, start_state, (query, inkey, values, log_forget))
    mean_square = lax.optimization_barrier(jnp.mean(recurrent * recurrent, axis=-1, keepdims=True))
    hidden = recurrent * lax.rsqrt(mean_square + eps_norm) * head_gain.reshape(HEADS, VAL_DIM)
    hidden = hidden.astype(jnp.bfloat16).reshape(length * sequences, HEADS * VAL_DIM)
    group_width = HEADS * VAL_DIM // N_TP
    total = jnp.zeros((length * sequences, D), jnp.float32)
    for group in range(N_TP):
        lower = group * group_width
        partial_value = jnp.dot(hidden[:, lower:lower + group_width], w_out[lower:lower + group_width], preferred_element_type=jnp.float32)
        total = total + lax.optimization_barrier(partial_value.astype(jnp.bfloat16)).astype(jnp.float32)
    return total.astype(jnp.bfloat16).reshape(length, sequences, D)
```

```python
import math

import jax
import jax.numpy as jnp
from jax import lax
from jax.sharding import Mesh
from jax.sharding import PartitionSpec as P

KEY_DIM = 128
VAL_DIM = 128
YT = ("y", "tp")

eps_norm = 1e-06


def exchanged(value, axis):
    return lax.all_to_all(value, axis, 0, 0, tiled=True)


def copies(value, count):
    return jnp.broadcast_to(value[None], (count, *value.shape))


def split_two(value):
    high = value.astype(jnp.bfloat16)
    low = (value - high.astype(jnp.float32)).astype(jnp.bfloat16)
    return high, low


def body(tokens, norm_gain, w_query, w_forget, w_value, floor_gap, head_gain, w_out):
    nz, ny, nt = (lax.axis_size(a) for a in ("z", "y", "tp"))
    pos, seqs, width = tokens.shape
    chunk = w_query.shape[0]
    key_width = w_query.shape[1]
    heads = key_width // KEY_DIM
    stretch = pos * ny * nt
    part = nz * chunk

    out_z = exchanged(copies(w_out, nz), "z")
    out_z = out_z.transpose(1, 0, 2).reshape(key_width, part)

    flat = tokens.astype(jnp.float32)
    scale = lax.rsqrt(jnp.mean(flat * flat, axis=-1, keepdims=True) + eps_norm)
    normed = (flat * scale * norm_gain).astype(jnp.bfloat16)
    by_y = normed.reshape(pos, seqs, nz, ny, chunk).transpose(3, 1, 0, 2, 4).reshape(ny, seqs, pos, part)
    send = jnp.broadcast_to(by_y[:, None], (ny, nt, seqs, pos, part)).reshape(ny * nt, seqs, pos, part)
    rows = exchanged(send, YT)

    weights = jnp.concatenate((w_forget, w_value, w_query), axis=1)
    weights = lax.all_gather(weights, "z", axis=0, tiled=True)
    rows = rows.transpose(1, 0, 2, 3).reshape(seqs, stretch, part)
    partial = jnp.einsum("sph,hd->spd", rows, weights, preferred_element_type=jnp.float32).astype(jnp.bfloat16)
    fv = exchanged(partial[..., : 2 * key_width], "y").astype(jnp.float32).sum(axis=0)
    fv = fv.astype(jnp.bfloat16)
    later = jnp.concatenate((partial[..., 2 * key_width :], copies(out_z, ny)), axis=2)
    later = exchanged(later, "y")
    query = later[..., :key_width].astype(jnp.float32).sum(axis=0).astype(jnp.bfloat16)
    out_rows = later[..., key_width:]

    forget = fv[:, :key_width].astype(jnp.float32)
    values = fv[:, key_width:].reshape(stretch, heads, VAL_DIM)
    inkey = floor_gap * jax.nn.sigmoid(-forget)
    log_forget = jnp.log1p(-inkey)
    positions = lax.iota(jnp.int32, stretch)
    causal = positions[:, None] >= positions[None, :]
    cumulative = jnp.dot(causal.astype(jnp.float32), log_forget, precision=lax.Precision.HIGHEST)
    final = cumulative[-1]
    key_final = (inkey * jnp.exp(final - cumulative)).astype(jnp.bfloat16).reshape(stretch, heads, KEY_DIM)
    end_state = jnp.einsum("uhk,uhv->hkv", key_final, values, preferred_element_type=jnp.float32)
    decay = jnp.exp(final)

    mine = heads * KEY_DIM // nz
    high, low = split_two(decay.reshape(nz, mine, 1))
    pieces = jnp.concatenate(
        (
            end_state.astype(jnp.bfloat16).reshape(nz, mine, VAL_DIM),
            jnp.broadcast_to(high, (nz, mine, 64)),
            jnp.broadcast_to(low, (nz, mine, 64)),
        ),
        axis=2,
    )
    pieces = exchanged(pieces, "z").astype(jnp.float32)
    state = jnp.zeros((mine, VAL_DIM), jnp.float32)
    entering = []
    for k in range(nz):
        entering.append(state.astype(jnp.bfloat16))
        factor = pieces[k, :, VAL_DIM : VAL_DIM + 1] + pieces[k, :, VAL_DIM + 64 : VAL_DIM + 65]
        state = factor * state + pieces[k, :, :VAL_DIM]
    incoming = exchanged(jnp.stack(entering), "z").reshape(heads, KEY_DIM, VAL_DIM)

    query = jax.nn.silu(query.astype(jnp.float32))
    query_scaled = (query * jnp.exp(cumulative)).astype(jnp.bfloat16).reshape(stretch, heads, KEY_DIM)
    key_scaled = (inkey * jnp.exp(-cumulative)).astype(jnp.bfloat16).reshape(stretch, heads, KEY_DIM)
    scores = jnp.einsum("thk,uhk->htu", query_scaled, key_scaled, preferred_element_type=jnp.float32)
    scores = jnp.where(causal, scores, 0.0).astype(jnp.bfloat16)
    recurrent = jnp.einsum("htu,uhv->thv", scores, values, preferred_element_type=jnp.float32)
    recurrent = recurrent + jnp.einsum("thk,hkv->thv", query_scaled, incoming, preferred_element_type=jnp.float32)
    mean_square = jnp.mean(recurrent * recurrent, axis=-1, keepdims=True)
    hidden = recurrent * lax.rsqrt(mean_square + eps_norm) * head_gain.reshape(heads, VAL_DIM)
    hidden = hidden.astype(jnp.bfloat16).reshape(stretch, heads * VAL_DIM)

    mixed = jnp.einsum("ph,yhd->pyd", hidden, out_rows, preferred_element_type=jnp.float32).astype(jnp.bfloat16)
    mixed = exchanged(mixed.reshape(ny * nt, pos, width), YT)
    mixed = mixed.reshape(seqs, nt, pos, width).astype(jnp.float32).sum(axis=1).astype(jnp.bfloat16)
    mixed = mixed.reshape(seqs, pos, ny, nz, chunk).transpose(1, 0, 3, 2, 4)
    return mixed.reshape(pos, seqs, width)


def solution(mesh):
    finer = Mesh(mesh.devices.reshape(16, 4, mesh.shape["tp"]), ("z", "y", "tp"))
    sp = ("z", "y")
    in_specs = (
        P(("z", "y", "tp"), None, None),
        P(),
        P(sp, "tp"),
        P(sp, "tp"),
        P(sp, "tp"),
        P("tp"),
        P("tp"),
        P("tp", sp),
    )
    out_specs = P(("z", "y", "tp"), None, None)
    return jax.shard_map(body, mesh=finer, in_specs=in_specs, out_specs=out_specs, check_vma=False)
```

```python
import jax
import jax.numpy as jnp
from jax import lax
from jax.experimental import pallas as pl
from jax.experimental.pallas import tpu as pltpu
from jax.sharding import Mesh
from jax.sharding import PartitionSpec as P


KEY_DIM = 128
VAL_DIM = 128
YT = ("y", "tp")
LANES = 128

eps_norm = 1e-06
f32 = jnp.float32
bf16 = jnp.bfloat16


def exchanged(value, axis):
    return lax.all_to_all(value, axis, 0, 0, tiled=True)


def copies(value, count):
    return jnp.broadcast_to(value[None], (count, *value.shape))


def call(kernel, out, flops, *args):
    outs = out if isinstance(out, (list, tuple)) else (out,)
    moved = sum(a.size * a.dtype.itemsize for a in args) + sum(o.size * o.dtype.itemsize for o in outs)
    return pl.pallas_call(
        kernel,
        out_shape=out,
        in_specs=[pl.BlockSpec(memory_space=pltpu.VMEM)] * len(args),
        out_specs=jax.tree.map(lambda _: pl.BlockSpec(memory_space=pltpu.VMEM), out),
        cost_estimate=pl.CostEstimate(flops=flops, bytes_accessed=moved, transcendentals=0),
        compiler_params=pltpu.CompilerParams(vmem_limit_bytes=16 * 1024 * 1024),
    )(*args)


def dot(a, b, dims):
    return lax.dot_general(a, b, (dims, ((), ())), preferred_element_type=f32)


def shuffled(blocks, chunk, source, rows):
    lane = lax.broadcasted_iota(jnp.int32, (rows, LANES), 1)
    result = None
    for j in range(LANES // chunk):
        block, group = source(j)
        shift = ((j - group) * chunk) % LANES
        moved = blocks(block)
        if shift:
            moved = pltpu.roll(moved, shift, 1)
        result = moved if result is None else jnp.where(lane >= j * chunk, moved, result)
    return result


def normalize_kernel(ny, nt, chunk, x_ref, gain_ref, out_ref):
    per = LANES // chunk
    rows, width = x_ref.shape
    x = x_ref[...].astype(f32)
    scale = lax.rsqrt(jnp.mean(x * x, axis=-1, keepdims=True) + eps_norm)
    normed = (x * scale * gain_ref[...]).astype(bf16).astype(f32)
    part = width // ny
    for y in range(ny):
        for q in range(part // LANES):

            def source(j):
                flat = ((q * per + j) * ny + y) * chunk
                return flat // LANES, (flat % LANES) // chunk

            block = shuffled(lambda b: normed[:, b * LANES : (b + 1) * LANES], chunk, source, rows).astype(bf16)
            for t in range(nt):
                out_ref[y, t, :, q * LANES : (q + 1) * LANES] = block


def split_parts(value):
    first = value.astype(bf16)
    rest = value - first.astype(f32)
    second = rest.astype(bf16)
    third = (rest - second.astype(f32)).astype(bf16)
    return first, second, third


def gates_kernel(fv_ref, gap_ref, piece_ref, sums_ref, inkey_ref, values_ref):
    ny, stretch, _ = fv_ref.shape
    width = gap_ref.shape[1]
    _, piece_rows, _ = piece_ref.shape
    mine = piece_rows - 8

    def total(lower):
        result = fv_ref[0, :, lower : lower + width].astype(f32)
        for k in range(1, ny):
            result = result + fv_ref[k, :, lower : lower + width].astype(f32)
        return result.astype(bf16)

    forget = total(0).astype(f32)
    values = total(width)
    values_ref[...] = values
    inkey = gap_ref[...] * jax.nn.sigmoid(-forget)
    log_forget = jnp.log1p(-inkey)
    row = lax.broadcasted_iota(jnp.int32, (stretch, stretch), 0)
    column = lax.broadcasted_iota(jnp.int32, (stretch, stretch), 1)
    causal = (row >= column).astype(bf16)
    parts = split_parts(log_forget)
    cumulative = sum(dot(causal, p, ((1,), (0,))) for p in parts)
    final = cumulative[stretch - 1 : stretch, :]
    sums_ref[...] = cumulative
    inkey_ref[...] = inkey
    key_final = (inkey * jnp.exp(final - cumulative)).astype(bf16)
    ones = jnp.ones((stretch, LANES), bf16)
    lane = lax.broadcasted_iota(jnp.int32, (8, LANES), 1)
    per_head = KEY_DIM // mine
    for h in range(width // KEY_DIM):
        cut = slice(h * KEY_DIM, (h + 1) * KEY_DIM)
        state = dot(key_final[:, cut], values[:, cut], ((0,), (0,))).astype(bf16)
        decay = jnp.exp(sum(dot(p[:, cut], ones, ((0,), (0,))) for p in parts))
        high = decay.astype(bf16).astype(f32)
        low = (decay - high).astype(bf16).astype(f32)
        for k in range(per_head):
            at = h * per_head + k
            lower = k * mine
            piece_ref[at, :mine, :] = state[lower : lower + mine]
            top = jnp.where(lane < 32, high[lower : lower + 8], low[lower : lower + 8])
            bottom = jnp.where(lane < 96, high[lower + 8 : lower + 16], low[lower + 8 : lower + 16])
            piece_ref[at, mine:, :] = jnp.where(lane < 64, top, bottom).astype(bf16)


def keys_kernel(sums_ref, inkey_ref, keys_ref):
    keys_ref[...] = (inkey_ref[...] * jnp.exp(-sums_ref[...])).astype(bf16)


def reach_kernel(sums_ref, reach_ref):
    reach_ref[...] = jnp.exp(sums_ref[...])


def prefix_kernel(piece_ref, out_ref):
    nz, mine, _ = out_ref.shape
    state = [jnp.zeros((8, VAL_DIM), f32) for _ in range(2)]
    for k in range(nz):
        out_ref[k] = jnp.concatenate(state, axis=0).astype(bf16)
        packed = piece_ref[k, mine:, :].astype(f32)
        added = piece_ref[k, :mine, :].astype(f32)
        for i in range(2):
            factor = packed[:, 64 * i : 64 * i + 1] + packed[:, 64 * i + 32 : 64 * i + 33]
            state[i] = factor * state[i] + added[8 * i : 8 * i + 8]


def inside_kernel(later_ref, reach_ref, keys_ref, values_ref, scaled_ref, inside_ref):
    ny = later_ref.shape[0]
    stretch, width = reach_ref.shape
    query = later_ref[0, :stretch, :].astype(f32)
    for k in range(1, ny):
        query = query + later_ref[k, :stretch, :].astype(f32)
    query = jax.nn.silu(query.astype(bf16).astype(f32))
    scaled = (query * reach_ref[...]).astype(bf16)
    scaled_ref[...] = scaled
    row = lax.broadcasted_iota(jnp.int32, (stretch, stretch), 0)
    column = lax.broadcasted_iota(jnp.int32, (stretch, stretch), 1)
    causal = row >= column
    for h in range(width // KEY_DIM):
        cut = slice(h * KEY_DIM, (h + 1) * KEY_DIM)
        scores = dot(scaled[:, cut], keys_ref[:, cut], ((1,), (1,)))
        scores = jnp.where(causal, scores, 0.0).astype(bf16)
        inside_ref[:, cut] = dot(scores, values_ref[:, cut], ((1,), (0,)))


def readout_kernel(later_ref, scaled_ref, inside_ref, state_ref, gain_ref, out_ref):
    ny = later_ref.shape[0]
    stretch, width = scaled_ref.shape
    hidden = []
    for h in range(width // KEY_DIM):
        cut = slice(h * KEY_DIM, (h + 1) * KEY_DIM)
        recurrent = inside_ref[:, cut] + dot(scaled_ref[:, cut], state_ref[cut, :], ((1,), (0,)))
        mean_square = jnp.mean(recurrent * recurrent, axis=-1, keepdims=True)
        hidden.append((recurrent * lax.rsqrt(mean_square + eps_norm) * gain_ref[:, cut]).astype(bf16))
    hidden = jnp.concatenate(hidden, axis=1)
    part = out_ref.shape[1] // ny
    for k in range(ny):
        out_ref[:, k * part : (k + 1) * part] = dot(hidden, later_ref[k, stretch:, :], ((1,), (1,))).astype(bf16)


def gather_kernel(nz, chunk, in_ref, out_ref):
    seqs, nt, pos, width = in_ref.shape
    ny = width // (nz * chunk)
    part = nz * chunk
    per = LANES // chunk
    for s in range(seqs):
        summed = in_ref[s, 0].astype(f32)
        for t in range(1, nt):
            summed = summed + in_ref[s, t].astype(f32)
        for b in range(width // LANES):

            def source(j):
                z, y = divmod(b * per + j, ny)
                flat = y * part + z * chunk
                return flat // LANES, (flat % LANES) // chunk

            block = shuffled(lambda k: summed[:, k * LANES : (k + 1) * LANES], chunk, source, pos)
            out_ref[s, :, b * LANES : (b + 1) * LANES] = block.astype(bf16)


def block(tokens, norm_gain, w_query, w_forget, w_value, floor_gap, head_gain, w_out):
    nz, ny, nt = (lax.axis_size(a) for a in ("z", "y", "tp"))
    pos, seqs, width = tokens.shape
    chunk, key_width = w_query.shape
    stretch = pos * ny * nt
    part = nz * chunk
    shape = jax.ShapeDtypeStruct

    ordered = tokens.transpose(1, 0, 2).reshape(seqs * pos, width)
    send = call(
        lambda *refs: normalize_kernel(ny, nt, chunk, *refs),
        shape((ny, nt, seqs * pos, part), bf16),
        1_000_000,
        ordered,
        norm_gain.reshape(1, width),
    )
    rows = exchanged(send.reshape(ny * nt, seqs, pos, part), YT)

    weights = jnp.concatenate((w_forget, w_value, w_query), axis=1)
    weights = lax.all_gather(weights, "z", axis=0, tiled=True)
    rows = rows.transpose(1, 0, 2, 3).reshape(seqs, stretch, part)

    def project(lower, upper):
        return jnp.einsum("sph,hd->spd", rows, weights[:, lower:upper], preferred_element_type=f32).astype(bf16)

    fv = exchanged(project(0, 2 * key_width), "y")
    out_z = exchanged(copies(w_out.T, nz), "z").reshape(part, key_width)
    later = jnp.concatenate((project(2 * key_width, 3 * key_width), copies(out_z, ny)), axis=1)
    later = exchanged(later, "y")

    mine = key_width // nz
    pieces, sums, inkey, values = call(
        gates_kernel,
        [
            shape((nz, mine + 8, VAL_DIM), bf16),
            shape((stretch, key_width), f32),
            shape((stretch, key_width), f32),
            shape((stretch, key_width), bf16),
        ],
        100_000_000,
        fv,
        floor_gap.reshape(1, key_width),
    )
    pieces = exchanged(pieces, "z")
    entering = call(prefix_kernel, shape((nz, mine, VAL_DIM), bf16), 1_000_000, pieces)
    incoming = exchanged(entering, "z").reshape(key_width, VAL_DIM)

    keys = call(keys_kernel, shape((stretch, key_width), bf16), 1_000_000, sums, inkey)
    reach = call(reach_kernel, shape((stretch, key_width), f32), 1_000_000, sums)
    scaled, inside = call(
        inside_kernel,
        [shape((stretch, key_width), bf16), shape((stretch, key_width), f32)],
        100_000_000,
        later,
        reach,
        keys,
        values,
    )
    mixed = call(
        readout_kernel,
        shape((stretch, width), bf16),
        300_000_000,
        later,
        scaled,
        inside,
        incoming,
        head_gain.reshape(1, key_width),
    )
    mixed = exchanged(mixed.reshape(ny * nt, pos, width), YT)
    mixed = call(
        lambda *refs: gather_kernel(nz, chunk, *refs),
        shape((seqs, pos, width), bf16),
        1_000_000,
        mixed.reshape(seqs, nt, pos, width),
    )
    return mixed.transpose(1, 0, 2)


def solution(mesh):
    finer = Mesh(mesh.devices.reshape(16, 4, mesh.shape["tp"]), ("z", "y", "tp"))
    sp = ("z", "y")
    in_specs = (
        P(("z", "y", "tp"), None, None),
        P(),
        P(sp, "tp"),
        P(sp, "tp"),
        P(sp, "tp"),
        P("tp"),
        P("tp"),
        P("tp", sp),
    )
    out_specs = P(("z", "y", "tp"), None, None)
    return jax.shard_map(block, mesh=finer, in_specs=in_specs, out_specs=out_specs, check_vma=False)
```

```python
import math

import jax
import jax.numpy as jnp
from jax import lax
from jax.experimental import pallas as pl
from jax.experimental.pallas import tpu as pltpu
from jax.sharding import Mesh
from jax.sharding import PartitionSpec as P


KEY_DIM = 128
VAL_DIM = 128
YT = ("y", "x", "c")
LANES = 128

eps_norm = 1e-06
f32 = jnp.float32
bf16 = jnp.bfloat16


def exchanged(value, axis):
    return lax.all_to_all(value, axis, 0, 0, tiled=True)


def call(kernel, out, flops, *args, scratch=()):
    outs = out if isinstance(out, (list, tuple)) else (out,)
    moved = sum(math.prod(a.shape) * jnp.dtype(a.dtype).itemsize for a in (*args, *outs))
    return pl.pallas_call(
        kernel,
        out_shape=out,
        in_specs=[pl.BlockSpec(memory_space=pltpu.SMEM if a.dtype == jnp.int32 else pltpu.VMEM) for a in args],
        out_specs=jax.tree.map(lambda _: pl.BlockSpec(memory_space=pltpu.VMEM), out),
        scratch_shapes=scratch,
        cost_estimate=pl.CostEstimate(flops=flops, bytes_accessed=moved, transcendentals=0),
        compiler_params=pltpu.CompilerParams(vmem_limit_bytes=16 * 1024 * 1024),
    )(*args)


def dot(a, b, dims):
    return lax.dot_general(a, b, (dims, ((), ())), preferred_element_type=f32)


def shuffled(blocks, chunk, source, rows):
    lane = lax.broadcasted_iota(jnp.int32, (rows, LANES), 1)
    result = None
    for j in range(LANES // chunk):
        block, group = source(j)
        shift = ((j - group) * chunk) % LANES
        moved = blocks(block)
        if shift:
            moved = pltpu.roll(moved, shift, 1)
        result = moved if result is None else jnp.where(lane >= j * chunk, moved, result)
    return result


def normalize_kernel(ny, nt, chunk, x_ref, gain_ref, *refs):
    *weight_refs, out_ref, packed_ref, row_ref = refs
    per = LANES // chunk
    pos, seqs, width = x_ref.shape
    at = 0
    for ref in weight_refs:
        for lower in range(0, ref.shape[1], LANES):
            rows = min(chunk, packed_ref.shape[0] - at)
            whole = rows // 8 * 8
            packed_ref[at : at + whole, :] = ref[:whole, lower : lower + LANES]
            if whole < rows:
                packed_ref[at + whole : at + rows, :] = ref[whole:rows, lower : lower + LANES]
            at += rows
    for p in range(pos):
        x = x_ref[p].astype(f32)
        scale = lax.rsqrt(jnp.mean(x * x, axis=-1, keepdims=True) + eps_norm)
        normed = (x * scale * gain_ref[...]).astype(bf16).astype(f32)
        for b in range(width // LANES):
            row_ref[b, pl.ds(p, seqs, stride=pos), :] = normed[:, b * LANES : (b + 1) * LANES]
    part = width // ny
    for y in range(ny):
        for q in range(part // LANES):

            def source(j):
                flat = ((q * per + j) * ny + y) * chunk
                return flat // LANES, (flat % LANES) // chunk

            block = shuffled(lambda b: row_ref[b], chunk, source, pos * seqs).astype(bf16)
            for t in range(nt):
                out_ref[y, t, :, q * LANES : (q + 1) * LANES] = block


def split_parts(value):
    first = value.astype(bf16)
    rest = value - first.astype(f32)
    second = rest.astype(bf16)
    third = (rest - second.astype(f32)).astype(bf16)
    return first, second, third


def joined(weights_ref, chunk, which):
    nz, _, lanes = weights_ref.shape
    halves = []
    for half in range(2):
        at = (2 * which + half) * chunk
        halves.append(weights_ref[:, at : at + chunk, :].reshape(nz * chunk, lanes))
    return jnp.concatenate(halves, axis=1)


def first_projection_kernel(rows_ref, weights_ref, out_t_ref, fv_ref):
    seqs = fv_ref.shape[0]
    sources, _, pos, part = rows_ref.shape
    stretch = sources * pos
    chunk, width = out_t_ref.shape
    rest = pltpu.roll(out_t_ref[chunk - 8 :, LANES:].astype(f32), 2, 0)
    rest = jnp.concatenate([rest, jnp.zeros((8, fv_ref.shape[2] - LANES), f32)], axis=1).astype(bf16)
    both = [joined(weights_ref, chunk, k) for k in range(2)]
    for s in range(seqs):
        rows = rows_ref[:, s].reshape(stretch, part)
        for k in range(2):
            fv_ref[s, :stretch, k * width : (k + 1) * width] = dot(rows, both[k], ((1,), (0,))).astype(bf16)
        fv_ref[s, stretch:, :] = rest


def put_out_rows(weights_ref, chunk, ref, base):
    nz = weights_ref.shape[0]
    first, second = 6 * chunk, 7 * chunk
    whole = chunk - 8
    for z in range(nz):
        at = base + z * chunk
        ref[at : at + chunk, :LANES] = weights_ref[z, first:second, :]
        ref[at : at + whole, LANES:] = weights_ref[z, second : second + whole, :]
        ref[at + whole : at + chunk, LANES:] = jnp.zeros((8, LANES), bf16)
        ref[at + whole : at + whole + 6, LANES:] = weights_ref[z, second + whole : second + whole + 6, :]


def second_projection_kernel(rows_ref, weights_ref, *out_refs):
    ny = len(out_refs)
    sources, _, pos, part = rows_ref.shape
    stretch = sources * pos
    chunk = part // weights_ref.shape[0]
    query = joined(weights_ref, chunk, 2)
    for d in range(ny):
        rows = rows_ref[:, lax.rem(lax.axis_index("y") + d, ny)].reshape(stretch, part)
        out_refs[d][:stretch, :] = dot(rows, query, ((1,), (0,))).astype(bf16)
        if out_refs[d].shape[0] > stretch:
            put_out_rows(weights_ref, chunk, out_refs[d], stretch)


def far_rows_kernel(chunk, weights_ref, far_ref):
    put_out_rows(weights_ref, chunk, far_ref, 0)


def whole_out_rows(ref, base, piece_ref, d, out_ref):
    nz, chunk, _ = out_ref.shape
    edge_row = lax.broadcasted_iota(jnp.int32, (8, LANES), 0)
    rest_at = piece_ref.shape[1] - 8
    for z in range(nz):
        at = base + z * chunk
        out_ref[z, :, :LANES] = ref[at : at + chunk, :LANES]
        out_ref[z, : chunk - 8, LANES:] = ref[at : at + chunk - 8, LANES:]
        moved = pltpu.roll(piece_ref[z, rest_at:, :].astype(f32), (6 - 2 * d) % 8, 0)
        old = ref[at + chunk - 8 : at + chunk, LANES:].astype(f32)
        out_ref[z, chunk - 8 :, LANES:] = jnp.where(edge_row >= 6, moved, old).astype(bf16)


def gates_kernel(fv_ref, gap_ref, piece_ref, sums_ref, inkey_ref, values_ref):
    ny = fv_ref.shape[0]
    stretch, width = sums_ref.shape
    nz = piece_ref.shape[0]
    mine = width // nz

    def total(lower):
        result = fv_ref[0, :stretch, lower : lower + width].astype(f32)
        for k in range(1, ny):
            result = result + fv_ref[k, :stretch, lower : lower + width].astype(f32)
        return result.astype(bf16)

    forget = total(0).astype(f32)
    values = total(width)
    values_ref[...] = values
    inkey = gap_ref[...] * jax.nn.sigmoid(-forget)
    log_forget = jnp.log1p(-inkey)
    row = lax.broadcasted_iota(jnp.int32, (stretch, stretch), 0)
    column = lax.broadcasted_iota(jnp.int32, (stretch, stretch), 1)
    causal = (row >= column).astype(bf16)
    parts = split_parts(log_forget)
    cumulative = sum(dot(causal, p, ((1,), (0,))) for p in parts)
    final = cumulative[stretch - 1 : stretch, :]
    sums_ref[...] = cumulative
    inkey_ref[...] = inkey
    key_final = (inkey * jnp.exp(final - cumulative)).astype(bf16)
    ones = jnp.ones((stretch, LANES), bf16)
    lane = lax.broadcasted_iota(jnp.int32, (8, LANES), 1)
    row = lax.broadcasted_iota(jnp.int32, (8, LANES), 0)
    rests = jnp.zeros((8, LANES), f32)
    for d in range(ny):
        source = lax.rem(lax.axis_index("y") + ny - d, ny)
        moved = fv_ref[source, stretch:, :LANES].astype(f32)
        rests = jnp.where(row // 2 == d, pltpu.roll(moved, 2 * d, 0) if d else moved, rests)
    rests = rests.astype(bf16)
    per_head = KEY_DIM // mine
    for h in range(width // KEY_DIM):
        cut = slice(h * KEY_DIM, (h + 1) * KEY_DIM)
        state = dot(key_final[:, cut], values[:, cut], ((0,), (0,))).astype(bf16)
        decay = jnp.exp(sum(dot(p[:, cut], ones, ((0,), (0,))) for p in parts))
        high = decay.astype(bf16).astype(f32)
        low = (decay - high).astype(bf16).astype(f32)
        for k in range(per_head):
            at = h * per_head + k
            lower = k * mine
            piece_ref[at, :mine, :] = state[lower : lower + mine]
            top = jnp.where(lane < 32, high[lower : lower + 8], low[lower : lower + 8])
            bottom = jnp.where(lane < 96, high[lower + 8 : lower + 16], low[lower + 8 : lower + 16])
            piece_ref[at, mine : mine + 8, :] = jnp.where(lane < 64, top, bottom).astype(bf16)
            piece_ref[at, mine + 8 :, :] = rests


def keys_kernel(sums_ref, inkey_ref, keys_ref):
    keys_ref[...] = (inkey_ref[...] * jnp.exp(-sums_ref[...])).astype(bf16)


def reach_kernel(sums_ref, reach_ref):
    reach_ref[...] = jnp.exp(sums_ref[...])


def prefix_kernel(piece_ref, out_ref):
    nz, mine, _ = out_ref.shape
    state = [jnp.zeros((8, VAL_DIM), f32) for _ in range(2)]
    for k in range(nz):
        out_ref[k] = jnp.concatenate(state, axis=0).astype(bf16)
        packed = piece_ref[k, mine : mine + 8, :].astype(f32)
        added = piece_ref[k, :mine, :].astype(f32)
        for i in range(2):
            factor = packed[:, 64 * i : 64 * i + 1] + packed[:, 64 * i + 32 : 64 * i + 33]
            state[i] = factor * state[i] + added[8 * i : 8 * i + 8]


def inside_kernel(*refs):
    *later_refs, reach_ref, keys_ref, values_ref, piece_ref, inside_ref, out_t_ref = refs
    stretch, width = reach_ref.shape
    query = later_refs[0][:stretch, :].astype(f32)
    for ref in later_refs[1:]:
        query = query + ref[:stretch, :].astype(f32)
    query = jax.nn.silu(query.astype(bf16).astype(f32))
    scaled = (query * reach_ref[...]).astype(bf16)
    inside_ref[:, width:] = scaled.astype(f32)
    row = lax.broadcasted_iota(jnp.int32, (stretch, stretch), 0)
    column = lax.broadcasted_iota(jnp.int32, (stretch, stretch), 1)
    causal = row >= column
    for h in range(width // KEY_DIM):
        cut = slice(h * KEY_DIM, (h + 1) * KEY_DIM)
        scores = dot(scaled[:, cut], keys_ref[:, cut], ((1,), (1,)))
        scores = jnp.where(causal, scores, 0.0).astype(bf16)
        inside_ref[:, cut] = dot(scores, values_ref[:, cut], ((1,), (0,)))
    for d, ref in enumerate(later_refs):
        if ref.shape[0] > stretch:
            whole_out_rows(ref, stretch, piece_ref, d, out_t_ref.at[d])


def merge_kernel(far, far_ref, piece_ref, out_ref):
    whole_out_rows(far_ref, 0, piece_ref, far, out_ref)


def readout_kernel(far, inside_ref, out_t_ref, far_out_ref, state_ref, gain_ref, give_ref, keep_ref):
    ny, nz, chunk, width = out_t_ref.shape
    stretch = inside_ref.shape[0]
    scaled = inside_ref[:, width:].astype(bf16)
    hidden = []
    for h in range(width // KEY_DIM):
        cut = slice(h * KEY_DIM, (h + 1) * KEY_DIM)
        recurrent = inside_ref[:, cut] + dot(scaled[:, cut], state_ref[cut, :], ((1,), (0,)))
        mean_square = jnp.mean(recurrent * recurrent, axis=-1, keepdims=True)
        hidden.append(recurrent * lax.rsqrt(mean_square + eps_norm) * gain_ref[:, cut])
    half = stretch // 2
    hidden = jnp.concatenate(hidden, axis=1).reshape(stretch // 16, 2, 8, width)
    first, second = (hidden[:, k].reshape(half, width) for k in range(2))
    at_first = lax.axis_index("c") == 0
    hidden = jnp.concatenate([jnp.where(at_first, second, first), jnp.where(at_first, first, second)], axis=0)
    hidden = hidden.astype(bf16)
    part = nz * chunk
    for d in range(ny):
        weight = (far_out_ref[...] if d == far else out_t_ref[d]).reshape(part, width)
        source = lax.rem(lax.axis_index("y") + ny - d, ny)
        columns = pl.ds(pl.multiple_of(source * part, part), part)
        mixed = dot(hidden, weight, ((1,), (1,))).astype(bf16)
        give_ref[:, columns] = mixed[:half]
        keep_ref[:, columns] = mixed[half:]


def pair_kernel(kept_ref, given_ref, out_ref):
    out_ref[...] = (kept_ref[...].astype(f32) + given_ref[...].astype(f32)).astype(bf16)


def gather_kernel(nz, chunk, in_ref, out_ref, row_ref):
    seqs, nt, pos, width = in_ref.shape
    ny = width // (nz * chunk)
    part = nz * chunk
    per = LANES // chunk
    for s in range(seqs):
        summed = in_ref[s, 0].astype(f32)
        for t in range(1, nt):
            summed = summed + in_ref[s, t].astype(f32)
        for b in range(width // LANES):

            def source(j):
                z, y = divmod(b * per + j, ny)
                flat = y * part + z * chunk
                return flat // LANES, (flat % LANES) // chunk

            block = shuffled(lambda k: summed[:, k * LANES : (k + 1) * LANES], chunk, source, pos)
            row_ref[b, s * pos : (s + 1) * pos, :] = block
    for p in range(pos):
        for b in range(width // LANES):
            rows = row_ref[b, pl.ds(p, seqs, stride=pos), :].astype(bf16)
            out_ref[p, :, b * LANES : (b + 1) * LANES] = rows


def block(tokens, norm_gain, w_query, w_forget, w_value, floor_gap, head_gain, w_out):
    nz, ny, nx, nc = (lax.axis_size(a) for a in ("z", "y", "x", "c"))
    nt = nx * nc
    pos, seqs, width = tokens.shape
    chunk, key_width = w_query.shape
    stretch = pos * ny * nt
    part = nz * chunk
    shape = jax.ShapeDtypeStruct

    out_t = w_out.T
    send, packed = call(
        lambda *refs: normalize_kernel(ny, nt, chunk, *refs),
        [
            pltpu.HBM((ny, nt, seqs * pos, part), bf16),
            shape((8 * chunk - 2, LANES), bf16),
        ],
        1_000_000,
        *(
            pltpu.with_memory_space_constraint(value, pltpu.MemorySpace.HBM)
            for value in (tokens, norm_gain.reshape(1, width), w_forget, w_value, w_query, out_t)
        ),
        scratch=[pltpu.VMEM((width // LANES, seqs * pos, LANES), f32)],
    )
    rows = exchanged(send.reshape(ny * nt, seqs, pos, part), YT)

    weights = lax.all_gather(packed, "z", axis=0)
    mine = key_width // nz
    far = ny // 2

    fv = call(
        first_projection_kernel, shape((seqs, stretch + 8, 2 * key_width), bf16), 550_000_000, rows, weights, out_t
    )
    fv = exchanged(fv, "y")
    pieces, sums, inkey, values = call(
        gates_kernel,
        [
            pltpu.HBM((nz, mine + 16, VAL_DIM), bf16),
            shape((stretch, key_width), f32),
            shape((stretch, key_width), f32),
            shape((stretch, key_width), bf16),
        ],
        100_000_000,
        fv,
        floor_gap.reshape(1, key_width),
    )
    pieces = exchanged(pieces, "z")
    sent = call(
        second_projection_kernel,
        [pltpu.HBM((stretch + (part if d != far else 0), key_width), bf16) for d in range(ny)],
        280_000_000,
        rows,
        weights,
    )

    def shifted(value, d):
        return lax.ppermute(value, "y", [(i, (i + d) % ny) for i in range(ny)])

    later = [sent[0]] + [shifted(sent[d], d) for d in range(1, ny)]
    far_out = call(lambda *refs: far_rows_kernel(chunk, *refs), pltpu.HBM((part, key_width), bf16), 1_000_000, weights)
    far_out = shifted(far_out, far)
    keys = call(keys_kernel, shape((stretch, key_width), bf16), 1_000_000, sums, inkey)
    reach = call(reach_kernel, shape((stretch, key_width), f32), 1_000_000, sums)
    entering = call(prefix_kernel, shape((nz, mine, VAL_DIM), bf16), 1_000_000, pieces)
    incoming = exchanged(entering, "z").reshape(key_width, VAL_DIM)
    inside, whole_out = call(
        inside_kernel,
        [
            shape((stretch, 2 * key_width), f32),
            shape((ny, nz, chunk, key_width), bf16),
        ],
        100_000_000,
        *later,
        reach,
        keys,
        values,
        pieces,
    )
    far_out = call(
        lambda *refs: merge_kernel(far, *refs), shape((nz, chunk, key_width), bf16), 1_000_000, far_out, pieces
    )
    give, kept = call(
        lambda *refs: readout_kernel(far, *refs),
        [pltpu.HBM((stretch // 2, width), bf16), shape((stretch // 2, width), bf16)],
        300_000_000,
        inside,
        whole_out,
        far_out,
        incoming,
        head_gain.reshape(1, key_width),
    )
    given = lax.ppermute(give, "c", [(0, 1), (1, 0)])
    mixed = call(pair_kernel, shape((stretch // 2, width), bf16), 1_000_000, kept, given)
    mixed = exchanged(mixed.reshape(ny * nx, pos, width), ("y", "x"))
    mixed = call(
        lambda *refs: gather_kernel(nz, chunk, *refs),
        shape((pos, seqs, width), bf16),
        1_000_000,
        mixed.reshape(seqs, nx, pos, width),
        scratch=[pltpu.VMEM((width // LANES, seqs * pos, LANES), f32)],
    )
    return mixed


def solution(mesh):
    finer = Mesh(mesh.devices.reshape(16, 4, 4, 2), ("z", "y", "x", "c"))
    sp, tp = ("z", "y"), ("x", "c")
    in_specs = (
        P((*sp, *tp), None, None),
        P(),
        P(sp, tp),
        P(sp, tp),
        P(sp, tp),
        P(tp),
        P(tp),
        P(tp, sp),
    )
    out_specs = P((*sp, *tp), None, None)
    return jax.shard_map(block, mesh=finer, in_specs=in_specs, out_specs=out_specs, check_vma=False)
```

```python
import math

import jax
import jax.numpy as jnp
from jax import lax
from jax.experimental import pallas as pl
from jax.experimental.pallas import tpu as pltpu
from jax.sharding import Mesh
from jax.sharding import PartitionSpec as P


KEY_DIM = 128
VAL_DIM = 128
YT = ("y", "x", "c")
LANES = 128

eps_norm = 1e-06
f32 = jnp.float32
bf16 = jnp.bfloat16


def exchanged(value, axis):
    return lax.all_to_all(value, axis, 0, 0, tiled=True)


def call(kernel, out, flops, *args, scratch=(), copied=()):
    outs = out if isinstance(out, (list, tuple)) else (out,)
    moved = sum(math.prod(a.shape) * jnp.dtype(a.dtype).itemsize for a in (*args, *outs))
    specs = [pl.BlockSpec(memory_space=pl.ANY if i in copied else pltpu.VMEM) for i in range(len(outs))]
    return pl.pallas_call(
        kernel,
        out_shape=out,
        in_specs=[pl.BlockSpec(memory_space=pltpu.SMEM if a.dtype == jnp.int32 else pltpu.VMEM) for a in args],
        out_specs=specs if isinstance(out, (list, tuple)) else specs[0],
        scratch_shapes=scratch,
        cost_estimate=pl.CostEstimate(flops=flops, bytes_accessed=moved, transcendentals=0),
        compiler_params=pltpu.CompilerParams(vmem_limit_bytes=16 * 1024 * 1024),
    )(*args)


def dot(a, b, dims):
    return lax.dot_general(a, b, (dims, ((), ())), preferred_element_type=f32)


def shuffled(blocks, chunk, source, rows):
    lane = lax.broadcasted_iota(jnp.int32, (rows, LANES), 1)
    result = None
    for j in range(LANES // chunk):
        block, group = source(j)
        shift = ((j - group) * chunk) % LANES
        moved = blocks(block)
        if shift:
            moved = pltpu.roll(moved, shift, 1)
        result = moved if result is None else jnp.where(lane >= j * chunk, moved, result)
    return result


def normalize_kernel(ny, nt, chunk, x_ref, gain_ref, *refs):
    *weight_refs, out_ref, packed_ref, row_ref = refs
    per = LANES // chunk
    pos, seqs, width = x_ref.shape
    at = 0
    for ref in weight_refs:
        for lower in range(0, ref.shape[1], LANES):
            rows = min(chunk, packed_ref.shape[0] - at)
            whole = rows // 8 * 8
            packed_ref[at : at + whole, :] = ref[:whole, lower : lower + LANES]
            if whole < rows:
                packed_ref[at + whole : at + rows, :] = ref[whole:rows, lower : lower + LANES]
            at += rows
    for p in range(pos):
        x = x_ref[p].astype(f32)
        scale = lax.rsqrt(jnp.mean(x * x, axis=-1, keepdims=True) + eps_norm)
        normed = (x * scale * gain_ref[...]).astype(bf16).astype(f32)
        for b in range(width // LANES):
            row_ref[b, pl.ds(p, seqs, stride=pos), :] = normed[:, b * LANES : (b + 1) * LANES]
    part = width // ny
    for y in range(ny):
        for q in range(part // LANES):

            def source(j):
                flat = ((q * per + j) * ny + y) * chunk
                return flat // LANES, (flat % LANES) // chunk

            block = shuffled(lambda b: row_ref[b], chunk, source, pos * seqs).astype(bf16)
            for t in range(nt):
                out_ref[y, t, :, q * LANES : (q + 1) * LANES] = block


def split_parts(value):
    first = value.astype(bf16)
    rest = value - first.astype(f32)
    second = rest.astype(bf16)
    third = (rest - second.astype(f32)).astype(bf16)
    return first, second, third


def joined(weights_ref, chunk, which):
    nz, _, lanes = weights_ref.shape
    halves = []
    for half in range(2):
        at = (2 * which + half) * chunk
        halves.append(weights_ref[:, at : at + chunk, :].reshape(nz * chunk, lanes))
    return jnp.concatenate(halves, axis=1)


def first_projection_kernel(rows_ref, weights_ref, out_t_ref, sent_ref, fv_ref, sems):
    seqs = fv_ref.shape[0]
    sources, _, pos, part = rows_ref.shape
    stretch = sources * pos
    chunk, width = out_t_ref.shape
    rest = pltpu.roll(out_t_ref[chunk - 8 :, LANES:].astype(f32), 1, 0)
    rest = jnp.concatenate([rest, jnp.zeros((8, fv_ref.shape[2] - LANES), f32)], axis=1).astype(bf16)
    both = [joined(weights_ref, chunk, k) for k in range(2)]
    for s in range(seqs):
        rows = rows_ref[:, s].reshape(stretch, part)
        for k in range(2):
            fv_ref[s, :stretch, k * width : (k + 1) * width] = dot(rows, both[k], ((1,), (0,))).astype(bf16)
        fv_ref[s, stretch:, :] = rest
        pltpu.make_async_copy(fv_ref.at[s], sent_ref.at[s], sems.at[s]).start()
    for s in range(seqs):
        pltpu.make_async_copy(fv_ref.at[s], sent_ref.at[s], sems.at[s]).wait()


def put_out_rows(weights_ref, chunk, ref, base):
    nz = weights_ref.shape[0]
    first, second = 6 * chunk, 7 * chunk
    whole = chunk - 8
    for z in range(nz):
        at = base + z * chunk
        ref[at : at + chunk, :LANES] = weights_ref[z, first:second, :]
        ref[at : at + whole, LANES:] = weights_ref[z, second : second + whole, :]
        ref[at + whole : at + chunk, LANES:] = jnp.zeros((8, LANES), bf16)
        ref[at + whole : at + whole + 7, LANES:] = weights_ref[z, second + whole : second + whole + 7, :]


def second_projection_kernel(rows_ref, weights_ref, *out_refs):
    ny = len(out_refs)
    sources, _, pos, part = rows_ref.shape
    stretch = sources * pos
    chunk = part // weights_ref.shape[0]
    query = joined(weights_ref, chunk, 2)
    for d in range(ny):
        rows = rows_ref[:, lax.rem(lax.axis_index("y") + d, ny)].reshape(stretch, part)
        out_refs[d][:stretch, :] = dot(rows, query, ((1,), (0,))).astype(bf16)
        if out_refs[d].shape[0] > stretch:
            put_out_rows(weights_ref, chunk, out_refs[d], stretch)


def far_rows_kernel(chunk, weights_ref, far_ref):
    put_out_rows(weights_ref, chunk, far_ref, 0)


def whole_out_rows(ref, base, piece_ref, d, out_ref):
    nz, chunk, _ = out_ref.shape
    edge_row = lax.broadcasted_iota(jnp.int32, (8, LANES), 0)
    rest_at = piece_ref.shape[1] - 8
    for z in range(nz):
        at = base + z * chunk
        out_ref[z, :, :LANES] = ref[at : at + chunk, :LANES]
        out_ref[z, : chunk - 8, LANES:] = ref[at : at + chunk - 8, LANES:]
        moved = pltpu.roll(piece_ref[z, rest_at:, :].astype(f32), 7 - d, 0)
        old = ref[at + chunk - 8 : at + chunk, LANES:].astype(f32)
        out_ref[z, chunk - 8 :, LANES:] = jnp.where(edge_row == 7, moved, old).astype(bf16)


def gates_kernel(fv_ref, gap_ref, piece_ref, sums_ref, inkey_ref, values_ref):
    ny = fv_ref.shape[0]
    stretch, width = sums_ref.shape
    nz = piece_ref.shape[0]
    mine = width // nz

    def total(lower):
        result = fv_ref[0, :stretch, lower : lower + width].astype(f32)
        for k in range(1, ny):
            result = result + fv_ref[k, :stretch, lower : lower + width].astype(f32)
        return result.astype(bf16)

    forget = total(0).astype(f32)
    values = total(width)
    values_ref[...] = values
    inkey = gap_ref[...] * jax.nn.sigmoid(-forget)
    log_forget = jnp.log1p(-inkey)
    row = lax.broadcasted_iota(jnp.int32, (stretch, stretch), 0)
    column = lax.broadcasted_iota(jnp.int32, (stretch, stretch), 1)
    causal = (row >= column).astype(bf16)
    parts = split_parts(log_forget)
    cumulative = sum(dot(causal, p, ((1,), (0,))) for p in parts)
    final = cumulative[stretch - 1 : stretch, :]
    sums_ref[...] = cumulative
    inkey_ref[...] = inkey
    key_final = (inkey * jnp.exp(final - cumulative)).astype(bf16)
    lane = lax.broadcasted_iota(jnp.int32, (8, LANES), 1)
    row = lax.broadcasted_iota(jnp.int32, (8, LANES), 0)
    rests = jnp.zeros((8, LANES), f32)
    for d in range(ny):
        source = lax.rem(lax.axis_index("y") + ny - d, ny)
        moved = fv_ref[source, stretch:, :LANES].astype(f32)
        rests = jnp.where(row == d, pltpu.roll(moved, d, 0) if d else moved, rests)
    per_head = KEY_DIM // mine
    for h in range(width // KEY_DIM):
        cut = slice(h * KEY_DIM, (h + 1) * KEY_DIM)
        state = dot(key_final[:, cut], values[:, cut], ((0,), (0,))).astype(bf16)
        decay = jnp.exp(jnp.broadcast_to(final[:, cut], (KEY_DIM, KEY_DIM)).T)
        high = decay.astype(bf16).astype(f32)
        low = (decay - high).astype(bf16).astype(f32)
        for k in range(per_head):
            at = h * per_head + k
            lower = k * mine
            piece_ref[at, :mine, :] = state[lower : lower + mine]
            tile = None
            for j in range(4):
                at8 = lower + 8 * (j // 2)
                both = jnp.where(lane % 32 < 16, high[at8 : at8 + 8], low[at8 : at8 + 8])
                both = both if j % 2 else pltpu.roll(both, 4, 0)
                tile = both if tile is None else jnp.where(lane < 32 * j, tile, both)
            piece_ref[at, mine:, :] = jnp.where(row < 4, rests, tile).astype(bf16)


def keys_kernel(sums_ref, inkey_ref, values_ref, both_ref):
    width = inkey_ref.shape[1]
    both_ref[:, :width] = (inkey_ref[...] * jnp.exp(-sums_ref[...])).astype(bf16)
    both_ref[:, width:] = values_ref[...]


def reach_kernel(sums_ref, reach_ref):
    reach_ref[...] = jnp.exp(sums_ref[...])


def prefix_kernel(piece_ref, out_ref):
    nz, mine, _ = out_ref.shape
    state = [jnp.zeros((4, VAL_DIM), f32) for _ in range(mine // 4)]
    for k in range(nz):
        out_ref[k] = jnp.concatenate(state, axis=0).astype(bf16)
        packed = piece_ref[k, mine:, :].astype(f32)[4:]
        added = piece_ref[k, :mine, :].astype(f32)
        for i in range(mine // 4):
            factor = packed[:, 32 * i : 32 * i + 1] + packed[:, 32 * i + 16 : 32 * i + 17]
            state[i] = factor * state[i] + added[4 * i : 4 * i + 4]


def inside_kernel(*refs):
    *later_refs, reach_ref, both_ref, piece_ref, inside_ref, out_t_ref = refs
    stretch, width = reach_ref.shape
    query = later_refs[0][:stretch, :].astype(f32)
    for ref in later_refs[1:]:
        query = query + ref[:stretch, :].astype(f32)
    query = jax.nn.silu(query.astype(bf16).astype(f32))
    scaled = (query * reach_ref[...]).astype(bf16)
    inside_ref[:, width:] = scaled.astype(f32)
    row = lax.broadcasted_iota(jnp.int32, (stretch, stretch), 0)
    column = lax.broadcasted_iota(jnp.int32, (stretch, stretch), 1)
    causal = row >= column
    for h in range(width // KEY_DIM):
        cut = slice(h * KEY_DIM, (h + 1) * KEY_DIM)
        scores = dot(scaled[:, cut], both_ref[:, cut], ((1,), (1,)))
        scores = jnp.where(causal, scores, 0.0).astype(bf16)
        inside_ref[:, cut] = dot(scores, both_ref[:, width + h * KEY_DIM : width + (h + 1) * KEY_DIM], ((1,), (0,)))
    for d, ref in enumerate(later_refs):
        if ref.shape[0] > stretch:
            whole_out_rows(ref, stretch, piece_ref, d, out_t_ref.at[d])


def merge_kernel(far, far_ref, piece_ref, out_ref):
    whole_out_rows(far_ref, 0, piece_ref, far, out_ref)


def readout_kernel(far, inside_ref, out_t_ref, far_out_ref, state_ref, gain_ref, *out_refs):
    sent_ref, keep_ref, give_ref, sems = out_refs
    ny, nz, chunk, width = out_t_ref.shape
    stretch = inside_ref.shape[0]
    scaled = inside_ref[:, width:].astype(bf16)
    hidden = []
    for h in range(width // KEY_DIM):
        cut = slice(h * KEY_DIM, (h + 1) * KEY_DIM)
        recurrent = inside_ref[:, cut] + dot(scaled[:, cut], state_ref[cut, :], ((1,), (0,)))
        mean_square = jnp.mean(recurrent * recurrent, axis=-1, keepdims=True)
        hidden.append(recurrent * lax.rsqrt(mean_square + eps_norm) * gain_ref[:, cut])
    half = stretch // 2
    hidden = jnp.concatenate(hidden, axis=1).reshape(stretch // 16, 2, 8, width)
    first, second = (hidden[:, k].reshape(half, width) for k in range(2))
    at_first = lax.axis_index("c") == 0
    hidden = jnp.concatenate([jnp.where(at_first, second, first), jnp.where(at_first, first, second)], axis=0)
    hidden = hidden.astype(bf16)
    part = nz * chunk
    for d in range(ny):
        weight = (far_out_ref[...] if d == far else out_t_ref[d]).reshape(part, width)
        source = lax.rem(lax.axis_index("y") + ny - d, ny)
        columns = pl.ds(pl.multiple_of(source * part, part), part)
        mixed = dot(hidden, weight, ((1,), (1,))).astype(bf16)
        keep_ref[:, columns] = mixed[half:]
        give_ref[d] = mixed[:half]
        pltpu.make_async_copy(give_ref.at[d], sent_ref.at[:, columns], sems.at[d]).start()
    for d in range(ny):
        source = lax.rem(lax.axis_index("y") + ny - d, ny)
        columns = pl.ds(pl.multiple_of(source * part, part), part)
        pltpu.make_async_copy(give_ref.at[d], sent_ref.at[:, columns], sems.at[d]).wait()


def pair_kernel(kept_ref, given_ref, out_ref):
    out_ref[...] = (kept_ref[...].astype(f32) + given_ref[...].astype(f32)).astype(bf16)


def gather_kernel(nz, chunk, in_ref, out_ref, row_ref):
    seqs, nt, pos, width = in_ref.shape
    ny = width // (nz * chunk)
    part = nz * chunk
    per = LANES // chunk
    for s in range(seqs):
        summed = in_ref[s, 0].astype(f32)
        for t in range(1, nt):
            summed = summed + in_ref[s, t].astype(f32)
        for b in range(width // LANES):

            def source(j):
                z, y = divmod(b * per + j, ny)
                flat = y * part + z * chunk
                return flat // LANES, (flat % LANES) // chunk

            block = shuffled(lambda k: summed[:, k * LANES : (k + 1) * LANES], chunk, source, pos)
            row_ref[b, s * pos : (s + 1) * pos, :] = block
    for p in range(pos):
        for b in range(width // LANES):
            rows = row_ref[b, pl.ds(p, seqs, stride=pos), :].astype(bf16)
            out_ref[p, :, b * LANES : (b + 1) * LANES] = rows


def block(tokens, norm_gain, w_query, w_forget, w_value, floor_gap, head_gain, w_out):
    nz, ny, nx, nc = (lax.axis_size(a) for a in ("z", "y", "x", "c"))
    nt = nx * nc
    pos, seqs, width = tokens.shape
    chunk, key_width = w_query.shape
    stretch = pos * ny * nt
    part = nz * chunk
    shape = jax.ShapeDtypeStruct

    out_t = w_out.T
    send, packed = call(
        lambda *refs: normalize_kernel(ny, nt, chunk, *refs),
        [
            pltpu.HBM((ny, nt, seqs * pos, part), bf16),
            shape((8 * chunk - 1, LANES), bf16),
        ],
        1_000_000,
        *(
            pltpu.with_memory_space_constraint(value, pltpu.MemorySpace.HBM)
            for value in (tokens, norm_gain.reshape(1, width), w_forget, w_value, w_query, out_t)
        ),
        scratch=[pltpu.VMEM((width // LANES, seqs * pos, LANES), f32)],
    )
    rows = exchanged(send.reshape(ny * nt, seqs, pos, part), YT)

    weights = lax.all_gather(packed, "z", axis=0)
    mine = key_width // nz
    far = ny // 2

    fv = call(
        first_projection_kernel,
        pltpu.HBM((seqs, stretch + 8, 2 * key_width), bf16),
        550_000_000,
        rows,
        weights,
        out_t,
        scratch=[pltpu.VMEM((seqs, stretch + 8, 2 * key_width), bf16), pltpu.SemaphoreType.DMA((seqs,))],
        copied=(0,),
    )
    fv = exchanged(fv, "y")
    pieces, sums, inkey, values = call(
        gates_kernel,
        [
            pltpu.HBM((nz, mine + 8, VAL_DIM), bf16),
            shape((stretch, key_width), f32),
            shape((stretch, key_width), f32),
            shape((stretch, key_width), bf16),
        ],
        100_000_000,
        fv,
        floor_gap.reshape(1, key_width),
    )
    pieces = exchanged(pieces, "z")
    sent = call(
        second_projection_kernel,
        [pltpu.HBM((stretch + (part if d != far else 0), key_width), bf16) for d in range(ny)],
        280_000_000,
        rows,
        weights,
    )

    def shifted(value, d):
        return lax.ppermute(value, "y", [(i, (i + d) % ny) for i in range(ny)])

    later = [sent[0]] + [shifted(sent[d], d) for d in range(1, ny)]
    far_out = call(lambda *refs: far_rows_kernel(chunk, *refs), pltpu.HBM((part, key_width), bf16), 1_000_000, weights)
    far_out = shifted(far_out, far)
    both = call(keys_kernel, shape((stretch, 2 * key_width), bf16), 1_000_000, sums, inkey, values)
    reach = call(reach_kernel, shape((stretch, key_width), f32), 1_000_000, sums)
    entering = call(prefix_kernel, shape((nz, mine, VAL_DIM), bf16), 1_000_000, pieces)
    incoming = exchanged(entering, "z").reshape(key_width, VAL_DIM)
    inside, whole_out = call(
        inside_kernel,
        [
            shape((stretch, 2 * key_width), f32),
            shape((ny, nz, chunk, key_width), bf16),
        ],
        100_000_000,
        *later,
        reach,
        both,
        pieces,
    )
    far_out = call(
        lambda *refs: merge_kernel(far, *refs), shape((nz, chunk, key_width), bf16), 1_000_000, far_out, pieces
    )
    give, kept = call(
        lambda *refs: readout_kernel(far, *refs),
        [pltpu.HBM((stretch // 2, width), bf16), shape((stretch // 2, width), bf16)],
        300_000_000,
        inside,
        whole_out,
        far_out,
        incoming,
        head_gain.reshape(1, key_width),
        scratch=[pltpu.VMEM((ny, stretch // 2, part), bf16), pltpu.SemaphoreType.DMA((ny,))],
        copied=(0,),
    )
    given = lax.ppermute(give, "c", [(0, 1), (1, 0)])
    mixed = call(pair_kernel, shape((stretch // 2, width), bf16), 1_000_000, kept, given)
    mixed = exchanged(mixed.reshape(ny * nx, pos, width), ("y", "x"))
    mixed = call(
        lambda *refs: gather_kernel(nz, chunk, *refs),
        shape((pos, seqs, width), bf16),
        1_000_000,
        mixed.reshape(seqs, nx, pos, width),
        scratch=[pltpu.VMEM((width // LANES, seqs * pos, LANES), f32)],
    )
    return mixed


def solution(mesh):
    finer = Mesh(mesh.devices.reshape(16, 4, 4, 2), ("z", "y", "x", "c"))
    sp, tp = ("z", "y"), ("x", "c")
    in_specs = (
        P((*sp, *tp), None, None),
        P(),
        P(sp, tp),
        P(sp, tp),
        P(sp, tp),
        P(tp),
        P(tp),
        P(tp, sp),
    )
    out_specs = P((*sp, *tp), None, None)
    return jax.shard_map(block, mesh=finer, in_specs=in_specs, out_specs=out_specs, check_vma=False)
```

```python
import math

import jax
import jax.numpy as jnp
from jax import lax
from jax.experimental import pallas as pl
from jax.experimental.pallas import tpu as pltpu
from jax.sharding import Mesh
from jax.sharding import PartitionSpec as P


KEY_DIM = 128
VAL_DIM = 128
YT = ("y", "x", "c")
LANES = 128

eps_norm = 1e-06
f32 = jnp.float32
bf16 = jnp.bfloat16


def exchanged(value, axis):
    return lax.all_to_all(value, axis, 0, 0, tiled=True)


def call(kernel, out, flops, *args, scratch=(), copied=()):
    outs = out if isinstance(out, (list, tuple)) else (out,)
    moved = sum(math.prod(a.shape) * jnp.dtype(a.dtype).itemsize for a in (*args, *outs))
    specs = [pl.BlockSpec(memory_space=pl.ANY if i in copied else pltpu.VMEM) for i in range(len(outs))]
    return pl.pallas_call(
        kernel,
        out_shape=out,
        in_specs=[pl.BlockSpec(memory_space=pltpu.SMEM if a.dtype == jnp.int32 else pltpu.VMEM) for a in args],
        out_specs=specs if isinstance(out, (list, tuple)) else specs[0],
        scratch_shapes=scratch,
        cost_estimate=pl.CostEstimate(flops=flops, bytes_accessed=moved, transcendentals=0),
        compiler_params=pltpu.CompilerParams(vmem_limit_bytes=16 * 1024 * 1024),
    )(*args)


def dot(a, b, dims):
    return lax.dot_general(a, b, (dims, ((), ())), preferred_element_type=f32)


def shuffled(blocks, chunk, source, rows):
    lane = lax.broadcasted_iota(jnp.int32, (rows, LANES), 1)
    result = None
    for j in range(LANES // chunk):
        block, group = source(j)
        shift = ((j - group) * chunk) % LANES
        moved = blocks(block)
        if shift:
            moved = pltpu.roll(moved, shift, 1)
        result = moved if result is None else jnp.where(lane >= j * chunk, moved, result)
    return result


def normalize_kernel(ny, nt, chunk, x_ref, gain_ref, *refs):
    *weight_refs, out_ref, packed_ref, row_ref = refs
    per = LANES // chunk
    pos, seqs, width = x_ref.shape
    at = 0
    for ref in weight_refs:
        for lower in range(0, ref.shape[1], LANES):
            rows = min(chunk, packed_ref.shape[0] - at)
            whole = rows // 8 * 8
            packed_ref[at : at + whole, :] = ref[:whole, lower : lower + LANES]
            if whole < rows:
                packed_ref[at + whole : at + rows, :] = ref[whole:rows, lower : lower + LANES]
            at += rows
    for p in range(pos):
        x = x_ref[p].astype(f32)
        scale = lax.rsqrt(jnp.mean(x * x, axis=-1, keepdims=True) + eps_norm)
        normed = (x * scale * gain_ref[...]).astype(bf16).astype(f32)
        for b in range(width // LANES):
            row_ref[b, pl.ds(p, seqs, stride=pos), :] = normed[:, b * LANES : (b + 1) * LANES]
    part = width // ny
    for y in range(ny):
        for q in range(part // LANES):

            def source(j):
                flat = ((q * per + j) * ny + y) * chunk
                return flat // LANES, (flat % LANES) // chunk

            block = shuffled(lambda b: row_ref[b], chunk, source, pos * seqs).astype(bf16)
            for t in range(nt):
                out_ref[y, t, :, q * LANES : (q + 1) * LANES] = block


def split_parts(value):
    first = value.astype(bf16)
    rest = value - first.astype(f32)
    second = rest.astype(bf16)
    third = (rest - second.astype(f32)).astype(bf16)
    return first, second, third


def joined(weights_ref, chunk, which):
    nz, _, lanes = weights_ref.shape
    halves = []
    for half in range(2):
        at = (2 * which + half) * chunk
        halves.append(weights_ref[:, at : at + chunk, :].reshape(nz * chunk, lanes))
    return jnp.concatenate(halves, axis=1)


def first_projection_kernel(rows_ref, weights_ref, out_t_ref, sent_ref, fv_ref, sems):
    seqs = fv_ref.shape[0]
    sources, _, pos, part = rows_ref.shape
    stretch = sources * pos
    chunk, width = out_t_ref.shape
    rest = pltpu.roll(out_t_ref[chunk - 8 :, LANES:].astype(f32), 1, 0)
    rest = jnp.concatenate([rest, jnp.zeros((8, fv_ref.shape[2] - LANES), f32)], axis=1).astype(bf16)
    both = [joined(weights_ref, chunk, k) for k in range(2)]
    for s in range(seqs):
        rows = rows_ref[:, s].reshape(stretch, part)
        for k in range(2):
            fv_ref[s, :stretch, k * width : (k + 1) * width] = dot(rows, both[k], ((1,), (0,))).astype(bf16)
        fv_ref[s, stretch:, :] = rest
        if s > 0:
            pltpu.make_async_copy(fv_ref.at[s - 1], sent_ref.at[s - 1], sems.at[s - 1]).start()
    pltpu.make_async_copy(fv_ref.at[seqs - 1], sent_ref.at[seqs - 1], sems.at[seqs - 1]).start()
    for s in range(seqs):
        pltpu.make_async_copy(fv_ref.at[s], sent_ref.at[s], sems.at[s]).wait()


def put_out_rows(weights_ref, chunk, ref, base):
    nz = weights_ref.shape[0]
    first, second = 6 * chunk, 7 * chunk
    whole = chunk - 8
    for z in range(nz):
        at = base + z * chunk
        ref[at : at + chunk, :LANES] = weights_ref[z, first:second, :]
        ref[at : at + whole, LANES:] = weights_ref[z, second : second + whole, :]
        ref[at + whole : at + chunk, LANES:] = jnp.zeros((8, LANES), bf16)
        ref[at + whole : at + whole + 7, LANES:] = weights_ref[z, second + whole : second + whole + 7, :]


def second_projection_kernel(rows_ref, weights_ref, *out_refs):
    ny = len(out_refs)
    sources, _, pos, part = rows_ref.shape
    stretch = sources * pos
    chunk = part // weights_ref.shape[0]
    query = joined(weights_ref, chunk, 2)
    for d in range(ny):
        rows = rows_ref[:, lax.rem(lax.axis_index("y") + d, ny)].reshape(stretch, part)
        out_refs[d][:stretch, :] = dot(rows, query, ((1,), (0,))).astype(bf16)
        if out_refs[d].shape[0] > stretch:
            put_out_rows(weights_ref, chunk, out_refs[d], stretch)


def far_rows_kernel(chunk, weights_ref, far_ref):
    put_out_rows(weights_ref, chunk, far_ref, 0)


def whole_out_rows(ref, base, piece_ref, d, out_ref):
    nz, chunk, _ = out_ref.shape
    edge_row = lax.broadcasted_iota(jnp.int32, (8, LANES), 0)
    rest_at = piece_ref.shape[1] - 8
    for z in range(nz):
        at = base + z * chunk
        out_ref[z, :, :LANES] = ref[at : at + chunk, :LANES]
        out_ref[z, : chunk - 8, LANES:] = ref[at : at + chunk - 8, LANES:]
        moved = pltpu.roll(piece_ref[z, rest_at:, :].astype(f32), 7 - d, 0)
        old = ref[at + chunk - 8 : at + chunk, LANES:].astype(f32)
        out_ref[z, chunk - 8 :, LANES:] = jnp.where(edge_row == 7, moved, old).astype(bf16)


def gates_kernel(fv_ref, gap_ref, piece_ref, sums_ref, inkey_ref, values_ref):
    ny = fv_ref.shape[0]
    stretch, width = sums_ref.shape
    nz = piece_ref.shape[0]
    mine = width // nz

    def total(lower):
        result = fv_ref[0, :stretch, lower : lower + width].astype(f32)
        for k in range(1, ny):
            result = result + fv_ref[k, :stretch, lower : lower + width].astype(f32)
        return result.astype(bf16)

    forget = total(0).astype(f32)
    values = total(width)
    values_ref[...] = values
    inkey = gap_ref[...] * jax.nn.sigmoid(-forget)
    log_forget = jnp.log1p(-inkey)
    row = lax.broadcasted_iota(jnp.int32, (stretch, stretch), 0)
    column = lax.broadcasted_iota(jnp.int32, (stretch, stretch), 1)
    causal = (row >= column).astype(bf16)
    parts = split_parts(log_forget)
    cumulative = sum(dot(causal, p, ((1,), (0,))) for p in parts)
    final = cumulative[stretch - 1 : stretch, :]
    sums_ref[...] = cumulative
    inkey_ref[...] = inkey
    key_final = (inkey * jnp.exp(final - cumulative)).astype(bf16)
    lane = lax.broadcasted_iota(jnp.int32, (8, LANES), 1)
    row = lax.broadcasted_iota(jnp.int32, (8, LANES), 0)
    rests = jnp.zeros((8, LANES), f32)
    for d in range(ny):
        source = lax.rem(lax.axis_index("y") + ny - d, ny)
        moved = fv_ref[source, stretch:, :LANES].astype(f32)
        rests = jnp.where(row == d, pltpu.roll(moved, d, 0) if d else moved, rests)
    per_head = KEY_DIM // mine
    for h in range(width // KEY_DIM):
        cut = slice(h * KEY_DIM, (h + 1) * KEY_DIM)
        state = dot(key_final[:, cut], values[:, cut], ((0,), (0,))).astype(bf16)
        decay = jnp.exp(jnp.broadcast_to(final[:, cut], (KEY_DIM, KEY_DIM)).T)
        high = decay.astype(bf16).astype(f32)
        low = (decay - high).astype(bf16).astype(f32)
        for k in range(per_head):
            at = h * per_head + k
            lower = k * mine
            piece_ref[at, :mine, :] = state[lower : lower + mine]
            tile = None
            for j in range(4):
                at8 = lower + 8 * (j // 2)
                both = jnp.where(lane % 32 < 16, high[at8 : at8 + 8], low[at8 : at8 + 8])
                both = both if j % 2 else pltpu.roll(both, 4, 0)
                tile = both if tile is None else jnp.where(lane < 32 * j, tile, both)
            piece_ref[at, mine:, :] = jnp.where(row < 4, rests, tile).astype(bf16)


def keys_kernel(sums_ref, inkey_ref, values_ref, both_ref):
    width = inkey_ref.shape[1]
    both_ref[:, :width] = (inkey_ref[...] * jnp.exp(-sums_ref[...])).astype(bf16)
    both_ref[:, width:] = values_ref[...]


def reach_kernel(sums_ref, reach_ref):
    reach_ref[...] = jnp.exp(sums_ref[...])


def prefix_kernel(piece_ref, out_ref):
    nz, mine, _ = out_ref.shape
    state = [jnp.zeros((4, VAL_DIM), f32) for _ in range(mine // 4)]
    for k in range(nz):
        out_ref[k] = jnp.concatenate(state, axis=0).astype(bf16)
        packed = piece_ref[k, mine:, :].astype(f32)[4:]
        added = piece_ref[k, :mine, :].astype(f32)
        for i in range(mine // 4):
            factor = packed[:, 32 * i : 32 * i + 1] + packed[:, 32 * i + 16 : 32 * i + 17]
            state[i] = factor * state[i] + added[4 * i : 4 * i + 4]


def inside_kernel(*refs):
    *later_refs, reach_ref, both_ref, piece_ref, inside_ref, out_t_ref = refs
    stretch, width = reach_ref.shape
    query = later_refs[0][:stretch, :].astype(f32)
    for ref in later_refs[1:]:
        query = query + ref[:stretch, :].astype(f32)
    query = jax.nn.silu(query.astype(bf16).astype(f32))
    scaled = (query * reach_ref[...]).astype(bf16)
    inside_ref[:, width:] = scaled.astype(f32)
    row = lax.broadcasted_iota(jnp.int32, (stretch, stretch), 0)
    column = lax.broadcasted_iota(jnp.int32, (stretch, stretch), 1)
    causal = row >= column
    for h in range(width // KEY_DIM):
        cut = slice(h * KEY_DIM, (h + 1) * KEY_DIM)
        scores = dot(scaled[:, cut], both_ref[:, cut], ((1,), (1,)))
        scores = jnp.where(causal, scores, 0.0).astype(bf16)
        inside_ref[:, cut] = dot(scores, both_ref[:, width + h * KEY_DIM : width + (h + 1) * KEY_DIM], ((1,), (0,)))
    for d, ref in enumerate(later_refs):
        if ref.shape[0] > stretch:
            whole_out_rows(ref, stretch, piece_ref, d, out_t_ref.at[d])


def merge_kernel(far, far_ref, piece_ref, out_ref):
    whole_out_rows(far_ref, 0, piece_ref, far, out_ref)


def readout_kernel(far, inside_ref, out_t_ref, far_out_ref, state_ref, gain_ref, *out_refs):
    sent_ref, keep_ref, give_ref, sems = out_refs
    ny, nz, chunk, width = out_t_ref.shape
    stretch = inside_ref.shape[0]
    scaled = inside_ref[:, width:].astype(bf16)
    hidden = []
    for h in range(width // KEY_DIM):
        cut = slice(h * KEY_DIM, (h + 1) * KEY_DIM)
        recurrent = inside_ref[:, cut] + dot(scaled[:, cut], state_ref[cut, :], ((1,), (0,)))
        mean_square = jnp.mean(recurrent * recurrent, axis=-1, keepdims=True)
        hidden.append(recurrent * lax.rsqrt(mean_square + eps_norm) * gain_ref[:, cut])
    half = stretch // 2
    hidden = jnp.concatenate(hidden, axis=1).reshape(stretch // 16, 2, 8, width)
    first, second = (hidden[:, k].reshape(half, width) for k in range(2))
    at_first = lax.axis_index("c") == 0
    hidden = jnp.concatenate([jnp.where(at_first, second, first), jnp.where(at_first, first, second)], axis=0)
    hidden = hidden.astype(bf16)
    part = nz * chunk

    def columns(d):
        source = lax.rem(lax.axis_index("y") + ny - d, ny)
        return pl.ds(pl.multiple_of(source * part, part), part)

    def copy(d):
        return pltpu.make_async_copy(give_ref.at[d], sent_ref.at[:, columns(d)], sems.at[d])

    for d in range(ny):
        weight = (far_out_ref[...] if d == far else out_t_ref[d]).reshape(part, width)
        mixed = dot(hidden, weight, ((1,), (1,))).astype(bf16)
        keep_ref[:, columns(d)] = mixed[half:]
        give_ref[d] = mixed[:half]
        if d > 0:
            copy(d - 1).start()
    copy(ny - 1).start()
    for d in range(ny):
        copy(d).wait()


def pair_kernel(kept_ref, given_ref, out_ref):
    out_ref[...] = (kept_ref[...].astype(f32) + given_ref[...].astype(f32)).astype(bf16)


def gather_kernel(nz, chunk, in_ref, out_ref, row_ref):
    seqs, nt, pos, width = in_ref.shape
    ny = width // (nz * chunk)
    part = nz * chunk
    per = LANES // chunk
    for s in range(seqs):
        summed = in_ref[s, 0].astype(f32)
        for t in range(1, nt):
            summed = summed + in_ref[s, t].astype(f32)
        for b in range(width // LANES):

            def source(j):
                z, y = divmod(b * per + j, ny)
                flat = y * part + z * chunk
                return flat // LANES, (flat % LANES) // chunk

            block = shuffled(lambda k: summed[:, k * LANES : (k + 1) * LANES], chunk, source, pos)
            row_ref[b, s * pos : (s + 1) * pos, :] = block
    for p in range(pos):
        for b in range(width // LANES):
            rows = row_ref[b, pl.ds(p, seqs, stride=pos), :].astype(bf16)
            out_ref[p, :, b * LANES : (b + 1) * LANES] = rows


def block(tokens, norm_gain, w_query, w_forget, w_value, floor_gap, head_gain, w_out):
    nz, ny, nx, nc = (lax.axis_size(a) for a in ("z", "y", "x", "c"))
    nt = nx * nc
    pos, seqs, width = tokens.shape
    chunk, key_width = w_query.shape
    stretch = pos * ny * nt
    part = nz * chunk
    shape = jax.ShapeDtypeStruct

    out_t = w_out.T
    send, packed = call(
        lambda *refs: normalize_kernel(ny, nt, chunk, *refs),
        [
            pltpu.HBM((ny, nt, seqs * pos, part), bf16),
            shape((8 * chunk - 1, LANES), bf16),
        ],
        1_000_000,
        *(
            pltpu.with_memory_space_constraint(value, pltpu.MemorySpace.HBM)
            for value in (tokens, norm_gain.reshape(1, width), w_forget, w_value, w_query, out_t)
        ),
        scratch=[pltpu.VMEM((width // LANES, seqs * pos, LANES), f32)],
    )
    rows = exchanged(send.reshape(ny * nt, seqs, pos, part), YT)

    weights = lax.all_gather(packed, "z", axis=0)
    mine = key_width // nz
    far = ny // 2

    fv = call(
        first_projection_kernel,
        pltpu.HBM((seqs, stretch + 8, 2 * key_width), bf16),
        550_000_000,
        rows,
        weights,
        out_t,
        scratch=[pltpu.VMEM((seqs, stretch + 8, 2 * key_width), bf16), pltpu.SemaphoreType.DMA((seqs,))],
        copied=(0,),
    )
    fv = exchanged(fv, "y")
    pieces, sums, inkey, values = call(
        gates_kernel,
        [
            pltpu.HBM((nz, mine + 8, VAL_DIM), bf16),
            shape((stretch, key_width), f32),
            shape((stretch, key_width), f32),
            shape((stretch, key_width), bf16),
        ],
        100_000_000,
        fv,
        floor_gap.reshape(1, key_width),
    )
    pieces = exchanged(pieces, "z")
    sent = call(
        second_projection_kernel,
        [pltpu.HBM((stretch + (part if d != far else 0), key_width), bf16) for d in range(ny)],
        280_000_000,
        rows,
        weights,
    )

    def shifted(value, d):
        return lax.ppermute(value, "y", [(i, (i + d) % ny) for i in range(ny)])

    later = [sent[0]] + [shifted(sent[d], d) for d in range(1, ny)]
    far_out = call(lambda *refs: far_rows_kernel(chunk, *refs), pltpu.HBM((part, key_width), bf16), 1_000_000, weights)
    far_out = shifted(far_out, far)
    both = call(keys_kernel, shape((stretch, 2 * key_width), bf16), 1_000_000, sums, inkey, values)
    reach = call(reach_kernel, shape((stretch, key_width), f32), 1_000_000, sums)
    entering = call(prefix_kernel, shape((nz, mine, VAL_DIM), bf16), 1_000_000, pieces)
    incoming = exchanged(entering, "z").reshape(key_width, VAL_DIM)
    inside, whole_out = call(
        inside_kernel,
        [
            shape((stretch, 2 * key_width), f32),
            shape((ny, nz, chunk, key_width), bf16),
        ],
        100_000_000,
        *later,
        reach,
        both,
        pieces,
    )
    far_out = call(
        lambda *refs: merge_kernel(far, *refs), shape((nz, chunk, key_width), bf16), 1_000_000, far_out, pieces
    )
    give, kept = call(
        lambda *refs: readout_kernel(far, *refs),
        [pltpu.HBM((stretch // 2, width), bf16), shape((stretch // 2, width), bf16)],
        300_000_000,
        inside,
        whole_out,
        far_out,
        incoming,
        head_gain.reshape(1, key_width),
        scratch=[pltpu.VMEM((ny, stretch // 2, part), bf16), pltpu.SemaphoreType.DMA((ny,))],
        copied=(0,),
    )
    given = lax.ppermute(give, "c", [(0, 1), (1, 0)])
    mixed = call(pair_kernel, shape((stretch // 2, width), bf16), 1_000_000, kept, given)
    mixed = exchanged(mixed.reshape(ny * nx, pos, width), ("y", "x"))
    mixed = call(
        lambda *refs: gather_kernel(nz, chunk, *refs),
        shape((pos, seqs, width), bf16),
        1_000_000,
        mixed.reshape(seqs, nx, pos, width),
        scratch=[pltpu.VMEM((width // LANES, seqs * pos, LANES), f32)],
    )
    return mixed


def solution(mesh):
    finer = Mesh(mesh.devices.reshape(16, 4, 4, 2), ("z", "y", "x", "c"))
    sp, tp = ("z", "y"), ("x", "c")
    in_specs = (
        P((*sp, *tp), None, None),
        P(),
        P(sp, tp),
        P(sp, tp),
        P(sp, tp),
        P(tp),
        P(tp),
        P(tp, sp),
    )
    out_specs = P((*sp, *tp), None, None)
    return jax.shard_map(block, mesh=finer, in_specs=in_specs, out_specs=out_specs, check_vma=False)
```

```python
import math

import jax
import jax.numpy as jnp
from jax import lax
from jax.experimental import pallas as pl
from jax.experimental.pallas import tpu as pltpu
from jax.sharding import Mesh
from jax.sharding import PartitionSpec as P


KEY_DIM = 128
VAL_DIM = 128
YT = ("y", "x", "c")
LANES = 128

eps_norm = 1e-06
f32 = jnp.float32
bf16 = jnp.bfloat16


def exchanged(value, axis):
    return lax.all_to_all(value, axis, 0, 0, tiled=True)


def call(kernel, out, flops, *args, scratch=(), copied=()):
    outs = out if isinstance(out, (list, tuple)) else (out,)
    moved = sum(math.prod(a.shape) * jnp.dtype(a.dtype).itemsize for a in (*args, *outs))
    specs = [pl.BlockSpec(memory_space=pl.ANY if i in copied else pltpu.VMEM) for i in range(len(outs))]
    return pl.pallas_call(
        kernel,
        out_shape=out,
        in_specs=[pl.BlockSpec(memory_space=pltpu.SMEM if a.dtype == jnp.int32 else pltpu.VMEM) for a in args],
        out_specs=specs if isinstance(out, (list, tuple)) else specs[0],
        scratch_shapes=scratch,
        cost_estimate=pl.CostEstimate(flops=flops, bytes_accessed=moved, transcendentals=0),
        compiler_params=pltpu.CompilerParams(vmem_limit_bytes=16 * 1024 * 1024),
    )(*args)


def dot(a, b, dims):
    return lax.dot_general(a, b, (dims, ((), ())), preferred_element_type=f32)


def shuffled(blocks, chunk, source, rows):
    lane = lax.broadcasted_iota(jnp.int32, (rows, LANES), 1)
    result = None
    for j in range(LANES // chunk):
        block, group = source(j)
        shift = ((j - group) * chunk) % LANES
        moved = blocks(block)
        if shift:
            moved = pltpu.roll(moved, shift, 1)
        result = moved if result is None else jnp.where(lane >= j * chunk, moved, result)
    return result


def normalize_kernel(ny, nt, chunk, x_ref, gain_ref, *refs):
    *weight_refs, out_ref, packed_ref, row_ref = refs
    per = LANES // chunk
    pos, seqs, width = x_ref.shape
    at = 0
    for ref in weight_refs:
        for lower in range(0, ref.shape[1], LANES):
            rows = min(chunk, packed_ref.shape[0] - at)
            whole = rows // 8 * 8
            packed_ref[at : at + whole, :] = ref[:whole, lower : lower + LANES]
            if whole < rows:
                packed_ref[at + whole : at + rows, :] = ref[whole:rows, lower : lower + LANES]
            at += rows
    for p in range(pos):
        x = x_ref[p].astype(f32)
        scale = lax.rsqrt(jnp.mean(x * x, axis=-1, keepdims=True) + eps_norm)
        normed = (x * scale * gain_ref[...]).astype(bf16).astype(f32)
        for b in range(width // LANES):
            row_ref[b, pl.ds(p, seqs, stride=pos), :] = normed[:, b * LANES : (b + 1) * LANES]
    part = width // ny
    for y in range(ny):
        for q in range(part // LANES):

            def source(j):
                flat = ((q * per + j) * ny + y) * chunk
                return flat // LANES, (flat % LANES) // chunk

            block = shuffled(lambda b: row_ref[b], chunk, source, pos * seqs).astype(bf16)
            for t in range(nt):
                out_ref[y, t, :, q * LANES : (q + 1) * LANES] = block


def split_parts(value):
    first = value.astype(bf16)
    rest = value - first.astype(f32)
    second = rest.astype(bf16)
    third = (rest - second.astype(f32)).astype(bf16)
    return first, second, third


def joined(weights_ref, chunk, which):
    nz, _, lanes = weights_ref.shape
    halves = []
    for half in range(2):
        at = (2 * which + half) * chunk
        halves.append(weights_ref[:, at : at + chunk, :].reshape(nz * chunk, lanes))
    return jnp.concatenate(halves, axis=1)


def first_projection_kernel(rows_ref, weights_ref, out_t_ref, sent_ref, fv_ref, sems):
    seqs = fv_ref.shape[0]
    sources, _, pos, part = rows_ref.shape
    stretch = sources * pos
    chunk, width = out_t_ref.shape
    rest = pltpu.roll(out_t_ref[chunk - 8 :, LANES:].astype(f32), 1, 0)
    rest = jnp.concatenate([rest, jnp.zeros((8, fv_ref.shape[2] - LANES), f32)], axis=1).astype(bf16)
    both = [joined(weights_ref, chunk, k) for k in range(2)]
    for s in range(seqs):
        rows = rows_ref[:, s].reshape(stretch, part)
        for k in range(2):
            fv_ref[s, :stretch, k * width : (k + 1) * width] = dot(rows, both[k], ((1,), (0,))).astype(bf16)
        fv_ref[s, stretch:, :] = rest
        if s > 0:
            pltpu.make_async_copy(fv_ref.at[s - 1], sent_ref.at[s - 1], sems.at[s - 1]).start()
    pltpu.make_async_copy(fv_ref.at[seqs - 1], sent_ref.at[seqs - 1], sems.at[seqs - 1]).start()
    for s in range(seqs):
        pltpu.make_async_copy(fv_ref.at[s], sent_ref.at[s], sems.at[s]).wait()


def put_out_rows(weights_ref, chunk, ref, base):
    nz = weights_ref.shape[0]
    first, second = 6 * chunk, 7 * chunk
    whole = chunk - 8
    for z in range(nz):
        at = base + z * chunk
        ref[at : at + chunk, :LANES] = weights_ref[z, first:second, :]
        ref[at : at + whole, LANES:] = weights_ref[z, second : second + whole, :]
        ref[at + whole : at + chunk, LANES:] = jnp.zeros((8, LANES), bf16)
        ref[at + whole : at + whole + 7, LANES:] = weights_ref[z, second + whole : second + whole + 7, :]


def second_projection_kernel(rows_ref, weights_ref, *out_refs):
    ny = len(out_refs)
    sources, _, pos, part = rows_ref.shape
    stretch = sources * pos
    chunk = part // weights_ref.shape[0]
    query = joined(weights_ref, chunk, 2)
    for d in range(ny):
        rows = rows_ref[:, lax.rem(lax.axis_index("y") + d, ny)].reshape(stretch, part)
        out_refs[d][:stretch, :] = dot(rows, query, ((1,), (0,))).astype(bf16)
        if out_refs[d].shape[0] > stretch:
            put_out_rows(weights_ref, chunk, out_refs[d], stretch)


def far_rows_kernel(chunk, weights_ref, far_ref):
    put_out_rows(weights_ref, chunk, far_ref, 0)


def whole_out_rows(ref, base, piece_ref, d, out_ref):
    nz, chunk, _ = out_ref.shape
    edge_row = lax.broadcasted_iota(jnp.int32, (8, LANES), 0)
    rest_at = piece_ref.shape[1] - 8
    for z in range(nz):
        at = base + z * chunk
        out_ref[z, :, :LANES] = ref[at : at + chunk, :LANES]
        out_ref[z, : chunk - 8, LANES:] = ref[at : at + chunk - 8, LANES:]
        moved = pltpu.roll(piece_ref[z, rest_at:, :].astype(f32), 7 - d, 0)
        old = ref[at + chunk - 8 : at + chunk, LANES:].astype(f32)
        out_ref[z, chunk - 8 :, LANES:] = jnp.where(edge_row == 7, moved, old).astype(bf16)


def gates_kernel(fv_ref, gap_ref, piece_ref, sums_ref, inkey_ref, values_ref):
    ny = fv_ref.shape[0]
    stretch, width = sums_ref.shape
    nz = piece_ref.shape[0]
    mine = width // nz

    def total(lower):
        result = fv_ref[0, :stretch, lower : lower + width].astype(f32)
        for k in range(1, ny):
            result = result + fv_ref[k, :stretch, lower : lower + width].astype(f32)
        return result.astype(bf16)

    forget = total(0).astype(f32)
    values = total(width)
    values_ref[...] = values
    inkey = gap_ref[...] * jax.nn.sigmoid(-forget)
    log_forget = jnp.log1p(-inkey)
    row = lax.broadcasted_iota(jnp.int32, (stretch, stretch), 0)
    column = lax.broadcasted_iota(jnp.int32, (stretch, stretch), 1)
    causal = (row >= column).astype(bf16)
    parts = split_parts(log_forget)
    cumulative = sum(dot(causal, p, ((1,), (0,))) for p in parts)
    final = cumulative[stretch - 1 : stretch, :]
    sums_ref[...] = cumulative
    inkey_ref[...] = inkey
    key_final = (inkey * jnp.exp(final - cumulative)).astype(bf16)
    lane = lax.broadcasted_iota(jnp.int32, (8, LANES), 1)
    row = lax.broadcasted_iota(jnp.int32, (8, LANES), 0)
    rests = jnp.zeros((8, LANES), f32)
    for d in range(ny):
        source = lax.rem(lax.axis_index("y") + ny - d, ny)
        moved = fv_ref[source, stretch:, :LANES].astype(f32)
        rests = jnp.where(row == d, pltpu.roll(moved, d, 0) if d else moved, rests)
    per_head = KEY_DIM // mine
    for h in range(width // KEY_DIM):
        cut = slice(h * KEY_DIM, (h + 1) * KEY_DIM)
        state = dot(key_final[:, cut], values[:, cut], ((0,), (0,))).astype(bf16)
        decay = jnp.exp(jnp.broadcast_to(final[:, cut], (KEY_DIM, KEY_DIM)).T)
        high = decay.astype(bf16).astype(f32)
        low = (decay - high).astype(bf16).astype(f32)
        for k in range(per_head):
            at = h * per_head + k
            lower = k * mine
            piece_ref[at, :mine, :] = state[lower : lower + mine]
            tile = None
            for j in range(4):
                at8 = lower + 8 * (j // 2)
                both = jnp.where(lane % 32 < 16, high[at8 : at8 + 8], low[at8 : at8 + 8])
                both = both if j % 2 else pltpu.roll(both, 4, 0)
                tile = both if tile is None else jnp.where(lane < 32 * j, tile, both)
            piece_ref[at, mine:, :] = jnp.where(row < 4, rests, tile).astype(bf16)


def keys_kernel(sums_ref, inkey_ref, values_ref, both_ref):
    width = inkey_ref.shape[1]
    both_ref[:, :width] = (inkey_ref[...] * jnp.exp(-sums_ref[...])).astype(bf16)
    both_ref[:, width:] = values_ref[...]


def reach_kernel(sums_ref, reach_ref):
    reach_ref[...] = jnp.exp(sums_ref[...])


def prefix_kernel(piece_ref, out_ref):
    nz, mine, _ = out_ref.shape
    state = [jnp.zeros((4, VAL_DIM), f32) for _ in range(mine // 4)]
    for k in range(nz):
        out_ref[k] = jnp.concatenate(state, axis=0).astype(bf16)
        packed = piece_ref[k, mine:, :].astype(f32)[4:]
        added = piece_ref[k, :mine, :].astype(f32)
        for i in range(mine // 4):
            factor = packed[:, 32 * i : 32 * i + 1] + packed[:, 32 * i + 16 : 32 * i + 17]
            state[i] = factor * state[i] + added[4 * i : 4 * i + 4]


def inside_kernel(*refs):
    *later_refs, reach_ref, both_ref, piece_ref, inside_ref, out_t_ref = refs
    stretch, width = reach_ref.shape
    query = later_refs[0][:stretch, :].astype(f32)
    for ref in later_refs[1:]:
        query = query + ref[:stretch, :].astype(f32)
    query = jax.nn.silu(query.astype(bf16).astype(f32))
    scaled = (query * reach_ref[...]).astype(bf16)
    inside_ref[:, width:] = scaled.astype(f32)
    row = lax.broadcasted_iota(jnp.int32, (stretch, stretch), 0)
    column = lax.broadcasted_iota(jnp.int32, (stretch, stretch), 1)
    causal = row >= column
    for h in range(width // KEY_DIM):
        cut = slice(h * KEY_DIM, (h + 1) * KEY_DIM)
        scores = dot(scaled[:, cut], both_ref[:, cut], ((1,), (1,)))
        scores = jnp.where(causal, scores, 0.0).astype(bf16)
        inside_ref[:, cut] = dot(scores, both_ref[:, width + h * KEY_DIM : width + (h + 1) * KEY_DIM], ((1,), (0,)))
    for d, ref in enumerate(later_refs):
        if ref.shape[0] > stretch:
            whole_out_rows(ref, stretch, piece_ref, d, out_t_ref.at[d])


def merge_kernel(far, far_ref, piece_ref, out_ref):
    whole_out_rows(far_ref, 0, piece_ref, far, out_ref)


def readout_kernel(far, inside_ref, out_t_ref, far_out_ref, state_ref, gain_ref, *out_refs):
    give_ref, keep_ref = out_refs
    ny, nz, chunk, width = out_t_ref.shape
    stretch = inside_ref.shape[0]
    scaled = inside_ref[:, width:].astype(bf16)
    hidden = []
    for h in range(width // KEY_DIM):
        cut = slice(h * KEY_DIM, (h + 1) * KEY_DIM)
        recurrent = inside_ref[:, cut] + dot(scaled[:, cut], state_ref[cut, :], ((1,), (0,)))
        mean_square = jnp.mean(recurrent * recurrent, axis=-1, keepdims=True)
        hidden.append(recurrent * lax.rsqrt(mean_square + eps_norm) * gain_ref[:, cut])
    half = stretch // 2
    hidden = jnp.concatenate(hidden, axis=1).reshape(stretch // 16, 2, 8, width)
    first, second = (hidden[:, k].reshape(half, width) for k in range(2))
    at_first = lax.axis_index("c") == 0
    hidden = jnp.concatenate([jnp.where(at_first, second, first), jnp.where(at_first, first, second)], axis=0)
    hidden = hidden.astype(bf16)
    part = nz * chunk

    def columns(d):
        source = lax.rem(lax.axis_index("y") + ny - d, ny)
        return pl.ds(pl.multiple_of(source * part, part), part)

    for d in range(ny):
        weight = (far_out_ref[...] if d == far else out_t_ref[d]).reshape(part, width)
        mixed = dot(hidden, weight, ((1,), (1,))).astype(bf16)
        keep_ref[:, columns(d)] = mixed[half:]
        give_ref[:, columns(d)] = mixed[:half]


def pair_kernel(kept_ref, given_ref, out_ref):
    out_ref[...] = (kept_ref[...].astype(f32) + given_ref[...].astype(f32)).astype(bf16)


def gather_kernel(nz, chunk, in_ref, out_ref, row_ref):
    seqs, nt, pos, width = in_ref.shape
    ny = width // (nz * chunk)
    part = nz * chunk
    per = LANES // chunk
    for s in range(seqs):
        summed = in_ref[s, 0].astype(f32)
        for t in range(1, nt):
            summed = summed + in_ref[s, t].astype(f32)
        for b in range(width // LANES):

            def source(j):
                z, y = divmod(b * per + j, ny)
                flat = y * part + z * chunk
                return flat // LANES, (flat % LANES) // chunk

            block = shuffled(lambda k: summed[:, k * LANES : (k + 1) * LANES], chunk, source, pos)
            row_ref[b, s * pos : (s + 1) * pos, :] = block
    for p in range(pos):
        for b in range(width // LANES):
            rows = row_ref[b, pl.ds(p, seqs, stride=pos), :].astype(bf16)
            out_ref[p, :, b * LANES : (b + 1) * LANES] = rows


def block(tokens, norm_gain, w_query, w_forget, w_value, floor_gap, head_gain, w_out):
    nz, ny, nx, nc = (lax.axis_size(a) for a in ("z", "y", "x", "c"))
    nt = nx * nc
    pos, seqs, width = tokens.shape
    chunk, key_width = w_query.shape
    stretch = pos * ny * nt
    part = nz * chunk
    shape = jax.ShapeDtypeStruct

    out_t = w_out.T
    send, packed = call(
        lambda *refs: normalize_kernel(ny, nt, chunk, *refs),
        [
            pltpu.HBM((ny, nt, seqs * pos, part), bf16),
            shape((8 * chunk - 1, LANES), bf16),
        ],
        1_000_000,
        *(
            pltpu.with_memory_space_constraint(value, pltpu.MemorySpace.HBM)
            for value in (tokens, norm_gain.reshape(1, width), w_forget, w_value, w_query, out_t)
        ),
        scratch=[pltpu.VMEM((width // LANES, seqs * pos, LANES), f32)],
    )
    rows = exchanged(send.reshape(ny * nt, seqs, pos, part), YT)

    weights = lax.all_gather(packed, "z", axis=0)
    mine = key_width // nz
    far = ny // 2

    fv = call(
        first_projection_kernel,
        pltpu.HBM((seqs, stretch + 8, 2 * key_width), bf16),
        550_000_000,
        rows,
        weights,
        out_t,
        scratch=[pltpu.VMEM((seqs, stretch + 8, 2 * key_width), bf16), pltpu.SemaphoreType.DMA((seqs,))],
        copied=(0,),
    )
    fv = exchanged(fv, "y")
    pieces, sums, inkey, values = call(
        gates_kernel,
        [
            pltpu.HBM((nz, mine + 8, VAL_DIM), bf16),
            shape((stretch, key_width), f32),
            shape((stretch, key_width), f32),
            shape((stretch, key_width), bf16),
        ],
        100_000_000,
        fv,
        floor_gap.reshape(1, key_width),
    )
    pieces = exchanged(pieces, "z")
    sent = call(
        second_projection_kernel,
        [pltpu.HBM((stretch + (part if d != far else 0), key_width), bf16) for d in range(ny)],
        280_000_000,
        rows,
        weights,
    )

    def shifted(value, d):
        return lax.ppermute(value, "y", [(i, (i + d) % ny) for i in range(ny)])

    later = [sent[0]] + [shifted(sent[d], d) for d in range(1, ny)]
    far_out = call(lambda *refs: far_rows_kernel(chunk, *refs), pltpu.HBM((part, key_width), bf16), 1_000_000, weights)
    far_out = shifted(far_out, far)
    both = call(keys_kernel, shape((stretch, 2 * key_width), bf16), 1_000_000, sums, inkey, values)
    reach = call(reach_kernel, shape((stretch, key_width), f32), 1_000_000, sums)
    entering = call(prefix_kernel, shape((nz, mine, VAL_DIM), bf16), 1_000_000, pieces)
    incoming = exchanged(entering, "z").reshape(key_width, VAL_DIM)
    inside, whole_out = call(
        inside_kernel,
        [
            shape((stretch, 2 * key_width), f32),
            shape((ny, nz, chunk, key_width), bf16),
        ],
        100_000_000,
        *later,
        reach,
        both,
        pieces,
    )
    far_out = call(
        lambda *refs: merge_kernel(far, *refs), shape((nz, chunk, key_width), bf16), 1_000_000, far_out, pieces
    )
    give, kept = call(
        lambda *refs: readout_kernel(far, *refs),
        [shape((stretch // 2, width), bf16)] * 2,
        300_000_000,
        inside,
        whole_out,
        far_out,
        incoming,
        head_gain.reshape(1, key_width),
    )
    given = lax.ppermute(give, "c", [(0, 1), (1, 0)])
    mixed = call(pair_kernel, shape((stretch // 2, width), bf16), 1_000_000, kept, given)
    mixed = exchanged(mixed.reshape(ny * nx, pos, width), ("y", "x"))
    mixed = call(
        lambda *refs: gather_kernel(nz, chunk, *refs),
        shape((pos, seqs, width), bf16),
        1_000_000,
        mixed.reshape(seqs, nx, pos, width),
        scratch=[pltpu.VMEM((width // LANES, seqs * pos, LANES), f32)],
    )
    return mixed


def solution(mesh):
    finer = Mesh(mesh.devices.reshape(16, 4, 4, 2), ("z", "y", "x", "c"))
    sp, tp = ("z", "y"), ("x", "c")
    in_specs = (
        P((*sp, *tp), None, None),
        P(),
        P(sp, tp),
        P(sp, tp),
        P(sp, tp),
        P(tp),
        P(tp),
        P(tp, sp),
    )
    out_specs = P((*sp, *tp), None, None)
    return jax.shard_map(block, mesh=finer, in_specs=in_specs, out_specs=out_specs, check_vma=False)
```

```python
import math

import jax
import jax.numpy as jnp
from jax import lax
from jax.experimental import pallas as pl
from jax.experimental.pallas import tpu as pltpu
from jax.sharding import Mesh
from jax.sharding import PartitionSpec as P


KEY_DIM = 128
VAL_DIM = 128
YT = ("y", "x", "c")
LANES = 128

eps_norm = 1e-06
f32 = jnp.float32
bf16 = jnp.bfloat16


def exchanged(value, axis):
    return lax.all_to_all(value, axis, 0, 0, tiled=True)


def call(kernel, out, flops, *args, scratch=(), copied=()):
    outs = out if isinstance(out, (list, tuple)) else (out,)
    moved = sum(math.prod(a.shape) * jnp.dtype(a.dtype).itemsize for a in (*args, *outs))
    specs = [pl.BlockSpec(memory_space=pl.ANY if i in copied else pltpu.VMEM) for i in range(len(outs))]
    return pl.pallas_call(
        kernel,
        out_shape=out,
        in_specs=[pl.BlockSpec(memory_space=pltpu.SMEM if a.dtype == jnp.int32 else pltpu.VMEM) for a in args],
        out_specs=specs if isinstance(out, (list, tuple)) else specs[0],
        scratch_shapes=scratch,
        cost_estimate=pl.CostEstimate(flops=flops, bytes_accessed=moved, transcendentals=0),
        compiler_params=pltpu.CompilerParams(vmem_limit_bytes=16 * 1024 * 1024),
    )(*args)


def dot(a, b, dims):
    return lax.dot_general(a, b, (dims, ((), ())), preferred_element_type=f32)


def shuffled(blocks, chunk, source, rows):
    lane = lax.broadcasted_iota(jnp.int32, (rows, LANES), 1)
    result = None
    for j in range(LANES // chunk):
        block, group = source(j)
        shift = ((j - group) * chunk) % LANES
        moved = blocks(block)
        if shift:
            moved = pltpu.roll(moved, shift, 1)
        result = moved if result is None else jnp.where(lane >= j * chunk, moved, result)
    return result


def normalize_kernel(ny, nt, chunk, x_ref, gain_ref, *refs):
    *weight_refs, out_ref, packed_ref, row_ref = refs
    per = LANES // chunk
    pos, seqs, width = x_ref.shape
    at = 0
    for ref in weight_refs:
        for lower in range(0, ref.shape[1], LANES):
            rows = min(chunk, packed_ref.shape[0] - at)
            whole = rows // 8 * 8
            packed_ref[at : at + whole, :] = ref[:whole, lower : lower + LANES]
            if whole < rows:
                packed_ref[at + whole : at + rows, :] = ref[whole:rows, lower : lower + LANES]
            at += rows
    for p in range(pos):
        x = x_ref[p].astype(f32)
        scale = lax.rsqrt(jnp.mean(x * x, axis=-1, keepdims=True) + eps_norm)
        normed = (x * scale * gain_ref[...]).astype(bf16).astype(f32)
        for b in range(width // LANES):
            row_ref[b, pl.ds(p, seqs, stride=pos), :] = normed[:, b * LANES : (b + 1) * LANES]
    part = width // ny
    for y in range(ny):
        for q in range(part // LANES):

            def source(j):
                flat = ((q * per + j) * ny + y) * chunk
                return flat // LANES, (flat % LANES) // chunk

            block = shuffled(lambda b: row_ref[b], chunk, source, pos * seqs).astype(bf16)
            for t in range(nt):
                out_ref[y, t, :, q * LANES : (q + 1) * LANES] = block


def split_parts(value):
    first = value.astype(bf16)
    rest = value - first.astype(f32)
    second = rest.astype(bf16)
    third = (rest - second.astype(f32)).astype(bf16)
    return first, second, third


def joined(weights_ref, chunk, which):
    nz, _, lanes = weights_ref.shape
    halves = []
    for half in range(2):
        at = (2 * which + half) * chunk
        halves.append(weights_ref[:, at : at + chunk, :].reshape(nz * chunk, lanes))
    return jnp.concatenate(halves, axis=1)


def first_projection_kernel(rows_ref, weights_ref, out_t_ref, sent_ref, fv_ref, sems):
    seqs = fv_ref.shape[0]
    sources, _, pos, part = rows_ref.shape
    stretch = sources * pos
    chunk, width = out_t_ref.shape
    rest = pltpu.roll(out_t_ref[chunk - 8 :, LANES:].astype(f32), 1, 0)
    rest = jnp.concatenate([rest, jnp.zeros((8, fv_ref.shape[2] - LANES), f32)], axis=1).astype(bf16)
    both = [joined(weights_ref, chunk, k) for k in range(2)]
    for s in range(seqs):
        rows = rows_ref[:, s].reshape(stretch, part)
        for k in range(2):
            fv_ref[s, :stretch, k * width : (k + 1) * width] = dot(rows, both[k], ((1,), (0,))).astype(bf16)
        fv_ref[s, stretch:, :] = rest
        if s > 0:
            pltpu.make_async_copy(fv_ref.at[s - 1], sent_ref.at[s - 1], sems.at[s - 1]).start()
    pltpu.make_async_copy(fv_ref.at[seqs - 1], sent_ref.at[seqs - 1], sems.at[seqs - 1]).start()
    for s in range(seqs):
        pltpu.make_async_copy(fv_ref.at[s], sent_ref.at[s], sems.at[s]).wait()


def put_out_rows(weights_ref, chunk, ref, base):
    nz = weights_ref.shape[0]
    first, second = 6 * chunk, 7 * chunk
    whole = chunk - 8
    for z in range(nz):
        at = base + z * chunk
        ref[at : at + chunk, :LANES] = weights_ref[z, first:second, :]
        ref[at : at + whole, LANES:] = weights_ref[z, second : second + whole, :]
        ref[at + whole : at + chunk, LANES:] = jnp.zeros((8, LANES), bf16)
        ref[at + whole : at + whole + 7, LANES:] = weights_ref[z, second + whole : second + whole + 7, :]


def second_projection_kernel(rows_ref, weights_ref, *out_refs):
    ny = len(out_refs)
    sources, _, pos, part = rows_ref.shape
    stretch = sources * pos
    chunk = part // weights_ref.shape[0]
    query = joined(weights_ref, chunk, 2)
    for d in range(ny):
        rows = rows_ref[:, lax.rem(lax.axis_index("y") + d, ny)].reshape(stretch, part)
        out_refs[d][:stretch, :] = dot(rows, query, ((1,), (0,))).astype(bf16)
        if out_refs[d].shape[0] > stretch:
            put_out_rows(weights_ref, chunk, out_refs[d], stretch)


def far_rows_kernel(chunk, weights_ref, far_ref):
    put_out_rows(weights_ref, chunk, far_ref, 0)


def whole_out_rows(ref, base, piece_ref, d, out_ref):
    nz, chunk, _ = out_ref.shape
    edge_row = lax.broadcasted_iota(jnp.int32, (8, LANES), 0)
    rest_at = piece_ref.shape[1] - 8
    for z in range(nz):
        at = base + z * chunk
        out_ref[z, :, :LANES] = ref[at : at + chunk, :LANES]
        out_ref[z, : chunk - 8, LANES:] = ref[at : at + chunk - 8, LANES:]
        moved = pltpu.roll(piece_ref[z, rest_at:, :].astype(f32), 7 - d, 0)
        old = ref[at + chunk - 8 : at + chunk, LANES:].astype(f32)
        out_ref[z, chunk - 8 :, LANES:] = jnp.where(edge_row == 7, moved, old).astype(bf16)


def gates_kernel(fv_ref, gap_ref, piece_ref, sums_ref, inkey_ref, values_ref):
    ny = fv_ref.shape[0]
    stretch, width = sums_ref.shape
    nz = piece_ref.shape[0]
    mine = width // nz

    def total(lower):
        result = fv_ref[0, :stretch, lower : lower + width].astype(f32)
        for k in range(1, ny):
            result = result + fv_ref[k, :stretch, lower : lower + width].astype(f32)
        return result.astype(bf16)

    forget = total(0).astype(f32)
    values = total(width)
    values_ref[...] = values
    inkey = gap_ref[...] * jax.nn.sigmoid(-forget)
    log_forget = jnp.log1p(-inkey)
    row = lax.broadcasted_iota(jnp.int32, (stretch, stretch), 0)
    column = lax.broadcasted_iota(jnp.int32, (stretch, stretch), 1)
    causal = (row >= column).astype(bf16)
    parts = split_parts(log_forget)
    cumulative = sum(dot(causal, p, ((1,), (0,))) for p in parts)
    final = cumulative[stretch - 1 : stretch, :]
    sums_ref[...] = cumulative
    inkey_ref[...] = inkey
    key_final = (inkey * jnp.exp(final - cumulative)).astype(bf16)
    lane = lax.broadcasted_iota(jnp.int32, (8, LANES), 1)
    row = lax.broadcasted_iota(jnp.int32, (8, LANES), 0)
    rests = jnp.zeros((8, LANES), f32)
    for d in range(ny):
        source = lax.rem(lax.axis_index("y") + ny - d, ny)
        moved = fv_ref[source, stretch:, :LANES].astype(f32)
        rests = jnp.where(row == d, pltpu.roll(moved, d, 0) if d else moved, rests)
    per_head = KEY_DIM // mine
    for h in range(width // KEY_DIM):
        cut = slice(h * KEY_DIM, (h + 1) * KEY_DIM)
        state = dot(key_final[:, cut], values[:, cut], ((0,), (0,))).astype(bf16)
        decay = jnp.exp(jnp.broadcast_to(final[:, cut], (KEY_DIM, KEY_DIM)).T)
        high = decay.astype(bf16).astype(f32)
        low = (decay - high).astype(bf16).astype(f32)
        for k in range(per_head):
            at = h * per_head + k
            lower = k * mine
            piece_ref[at, :mine, :] = state[lower : lower + mine]
            tile = None
            for j in range(4):
                at8 = lower + 8 * (j // 2)
                both = jnp.where(lane % 32 < 16, high[at8 : at8 + 8], low[at8 : at8 + 8])
                both = both if j % 2 else pltpu.roll(both, 4, 0)
                tile = both if tile is None else jnp.where(lane < 32 * j, tile, both)
            piece_ref[at, mine:, :] = jnp.where(row < 4, rests, tile).astype(bf16)


def keys_kernel(sums_ref, inkey_ref, values_ref, both_ref):
    width = inkey_ref.shape[1]
    both_ref[:, :width] = (inkey_ref[...] * jnp.exp(-sums_ref[...])).astype(bf16)
    both_ref[:, width:] = values_ref[...]


def reach_kernel(sums_ref, reach_ref):
    reach_ref[...] = jnp.exp(sums_ref[...])


def prefix_kernel(piece_ref, out_ref):
    nz, mine, _ = out_ref.shape
    state = [jnp.zeros((4, VAL_DIM), f32) for _ in range(mine // 4)]
    for k in range(nz):
        out_ref[k] = jnp.concatenate(state, axis=0).astype(bf16)
        packed = piece_ref[k, mine:, :].astype(f32)[4:]
        added = piece_ref[k, :mine, :].astype(f32)
        for i in range(mine // 4):
            factor = packed[:, 32 * i : 32 * i + 1] + packed[:, 32 * i + 16 : 32 * i + 17]
            state[i] = factor * state[i] + added[4 * i : 4 * i + 4]


def inside_kernel(*refs):
    *later_refs, reach_ref, both_ref, piece_ref, inside_ref, out_t_ref = refs
    stretch, width = reach_ref.shape
    query = later_refs[0][:stretch, :].astype(f32)
    for ref in later_refs[1:]:
        query = query + ref[:stretch, :].astype(f32)
    query = jax.nn.silu(query.astype(bf16).astype(f32))
    scaled = (query * reach_ref[...]).astype(bf16)
    inside_ref[:, width:] = scaled.astype(f32)
    row = lax.broadcasted_iota(jnp.int32, (stretch, stretch), 0)
    column = lax.broadcasted_iota(jnp.int32, (stretch, stretch), 1)
    causal = row >= column
    for h in range(width // KEY_DIM):
        cut = slice(h * KEY_DIM, (h + 1) * KEY_DIM)
        scores = dot(scaled[:, cut], both_ref[:, cut], ((1,), (1,)))
        scores = jnp.where(causal, scores, 0.0).astype(bf16)
        inside_ref[:, cut] = dot(scores, both_ref[:, width + h * KEY_DIM : width + (h + 1) * KEY_DIM], ((1,), (0,)))
    for d, ref in enumerate(later_refs):
        if ref.shape[0] > stretch:
            whole_out_rows(ref, stretch, piece_ref, d, out_t_ref.at[d])


def merge_kernel(far, far_ref, piece_ref, out_ref):
    whole_out_rows(far_ref, 0, piece_ref, far, out_ref)


def readout_kernel(far, inside_ref, out_t_ref, far_out_ref, state_ref, gain_ref, *out_refs):
    give_ref, kept_ref = out_refs
    _, _, _, width = out_t_ref.shape
    stretch = inside_ref.shape[0]
    scaled = inside_ref[:, width:].astype(bf16)
    hidden = []
    for h in range(width // KEY_DIM):
        cut = slice(h * KEY_DIM, (h + 1) * KEY_DIM)
        recurrent = inside_ref[:, cut] + dot(scaled[:, cut], state_ref[cut, :], ((1,), (0,)))
        mean_square = jnp.mean(recurrent * recurrent, axis=-1, keepdims=True)
        hidden.append(recurrent * lax.rsqrt(mean_square + eps_norm) * gain_ref[:, cut])
    half = stretch // 2
    hidden = jnp.concatenate(hidden, axis=1).reshape(stretch // 16, 2, 8, width)
    first, second = (hidden[:, k].reshape(half, width) for k in range(2))
    at_first = lax.axis_index("c") == 0
    kept_ref[...] = jnp.where(at_first, first, second).astype(bf16)
    write_mixed(far, jnp.where(at_first, second, first).astype(bf16), out_t_ref, far_out_ref, give_ref)


def write_mixed(far, hidden, out_t_ref, far_out_ref, out_ref):
    ny, nz, chunk, width = out_t_ref.shape
    part = nz * chunk
    for d in range(ny):
        weight = (far_out_ref[...] if d == far else out_t_ref[d]).reshape(part, width)
        source = lax.rem(lax.axis_index("y") + ny - d, ny)
        columns = pl.ds(pl.multiple_of(source * part, part), part)
        out_ref[:, columns] = dot(hidden, weight, ((1,), (1,))).astype(bf16)


def keep_kernel(far, kept_ref, out_t_ref, far_out_ref, out_ref):
    write_mixed(far, kept_ref[...], out_t_ref, far_out_ref, out_ref)


def pair_kernel(kept_ref, given_ref, out_ref):
    out_ref[...] = (kept_ref[...].astype(f32) + given_ref[...].astype(f32)).astype(bf16)


def gather_kernel(nz, chunk, in_ref, out_ref, row_ref):
    seqs, nt, pos, width = in_ref.shape
    ny = width // (nz * chunk)
    part = nz * chunk
    per = LANES // chunk
    for s in range(seqs):
        summed = in_ref[s, 0].astype(f32)
        for t in range(1, nt):
            summed = summed + in_ref[s, t].astype(f32)
        for b in range(width // LANES):

            def source(j):
                z, y = divmod(b * per + j, ny)
                flat = y * part + z * chunk
                return flat // LANES, (flat % LANES) // chunk

            block = shuffled(lambda k: summed[:, k * LANES : (k + 1) * LANES], chunk, source, pos)
            row_ref[b, s * pos : (s + 1) * pos, :] = block
    for p in range(pos):
        for b in range(width // LANES):
            rows = row_ref[b, pl.ds(p, seqs, stride=pos), :].astype(bf16)
            out_ref[p, :, b * LANES : (b + 1) * LANES] = rows


def block(tokens, norm_gain, w_query, w_forget, w_value, floor_gap, head_gain, w_out):
    nz, ny, nx, nc = (lax.axis_size(a) for a in ("z", "y", "x", "c"))
    nt = nx * nc
    pos, seqs, width = tokens.shape
    chunk, key_width = w_query.shape
    stretch = pos * ny * nt
    part = nz * chunk
    shape = jax.ShapeDtypeStruct

    out_t = w_out.T
    send, packed = call(
        lambda *refs: normalize_kernel(ny, nt, chunk, *refs),
        [
            pltpu.HBM((ny, nt, seqs * pos, part), bf16),
            shape((8 * chunk - 1, LANES), bf16),
        ],
        1_000_000,
        *(
            pltpu.with_memory_space_constraint(value, pltpu.MemorySpace.HBM)
            for value in (tokens, norm_gain.reshape(1, width), w_forget, w_value, w_query, out_t)
        ),
        scratch=[pltpu.VMEM((width // LANES, seqs * pos, LANES), f32)],
    )
    rows = exchanged(send.reshape(ny * nt, seqs, pos, part), YT)

    weights = lax.all_gather(packed, "z", axis=0)
    mine = key_width // nz
    far = ny // 2

    fv = call(
        first_projection_kernel,
        pltpu.HBM((seqs, stretch + 8, 2 * key_width), bf16),
        550_000_000,
        rows,
        weights,
        out_t,
        scratch=[pltpu.VMEM((seqs, stretch + 8, 2 * key_width), bf16), pltpu.SemaphoreType.DMA((seqs,))],
        copied=(0,),
    )
    fv = exchanged(fv, "y")
    pieces, sums, inkey, values = call(
        gates_kernel,
        [
            pltpu.HBM((nz, mine + 8, VAL_DIM), bf16),
            shape((stretch, key_width), f32),
            shape((stretch, key_width), f32),
            shape((stretch, key_width), bf16),
        ],
        100_000_000,
        fv,
        floor_gap.reshape(1, key_width),
    )
    pieces = exchanged(pieces, "z")
    sent = call(
        second_projection_kernel,
        [pltpu.HBM((stretch + (part if d != far else 0), key_width), bf16) for d in range(ny)],
        280_000_000,
        rows,
        weights,
    )

    def shifted(value, d):
        return lax.ppermute(value, "y", [(i, (i + d) % ny) for i in range(ny)])

    later = [sent[0]] + [shifted(sent[d], d) for d in range(1, ny)]
    far_out = call(lambda *refs: far_rows_kernel(chunk, *refs), pltpu.HBM((part, key_width), bf16), 1_000_000, weights)
    far_out = shifted(far_out, far)
    both = call(keys_kernel, shape((stretch, 2 * key_width), bf16), 1_000_000, sums, inkey, values)
    reach = call(reach_kernel, shape((stretch, key_width), f32), 1_000_000, sums)
    entering = call(prefix_kernel, shape((nz, mine, VAL_DIM), bf16), 1_000_000, pieces)
    incoming = exchanged(entering, "z").reshape(key_width, VAL_DIM)
    inside, whole_out = call(
        inside_kernel,
        [
            shape((stretch, 2 * key_width), f32),
            shape((ny, nz, chunk, key_width), bf16),
        ],
        100_000_000,
        *later,
        reach,
        both,
        pieces,
    )
    far_out = call(
        lambda *refs: merge_kernel(far, *refs), shape((nz, chunk, key_width), bf16), 1_000_000, far_out, pieces
    )
    give, kept = call(
        lambda *refs: readout_kernel(far, *refs),
        [shape((stretch // 2, width), bf16), shape((stretch // 2, key_width), bf16)],
        300_000_000,
        inside,
        whole_out,
        far_out,
        incoming,
        head_gain.reshape(1, key_width),
    )
    given = lax.ppermute(give, "c", [(0, 1), (1, 0)])
    kept = call(
        lambda *refs: keep_kernel(far, *refs), shape((stretch // 2, width), bf16), 150_000_000, kept, whole_out, far_out
    )
    mixed = call(pair_kernel, shape((stretch // 2, width), bf16), 1_000_000, kept, given)
    mixed = exchanged(mixed.reshape(ny * nx, pos, width), ("y", "x"))
    mixed = call(
        lambda *refs: gather_kernel(nz, chunk, *refs),
        shape((pos, seqs, width), bf16),
        1_000_000,
        mixed.reshape(seqs, nx, pos, width),
        scratch=[pltpu.VMEM((width // LANES, seqs * pos, LANES), f32)],
    )
    return mixed


def solution(mesh):
    finer = Mesh(mesh.devices.reshape(16, 4, 4, 2), ("z", "y", "x", "c"))
    sp, tp = ("z", "y"), ("x", "c")
    in_specs = (
        P((*sp, *tp), None, None),
        P(),
        P(sp, tp),
        P(sp, tp),
        P(sp, tp),
        P(tp),
        P(tp),
        P(tp, sp),
    )
    out_specs = P((*sp, *tp), None, None)
    return jax.shard_map(block, mesh=finer, in_specs=in_specs, out_specs=out_specs, check_vma=False)
```
